32 devices in a mesh: ep: 8 (over z, core), tp: 4 (over y, x).
Axes of the slice: x: 2, y: 2, z: 4, core: 2. Of those that a mesh axis runs over, the one named last changes fastest.
Arguments:
- mixer_input: bfloat16 [2048, 1024], P('ep', 'tp'), may hold values from -6 to 6
- log_step: float32 [64], P('tp'), may hold values from -12.8 to -2.7
- decay_shift: float32 [2048, 64], P('ep', 'tp'), may hold values from -2 to 0
- input_map: bfloat16 [2, 64, 64, 16], P(None, 'tp'), may hold values from -71.55418 to 71.55418
- readout: float32 [2, 64, 16, 64], P(None, 'tp'), may hold values from -0.5 to 0.5
- mixer_weight: bfloat16 [1024, 2048], P(None, 'tp'), may hold values from -0.1875 to 0.1875
- expert_input: bfloat16 [1024, 2048], P('ep'), may hold values from -6 to 6
- norm_gain: float32 [2048], replicated, may hold values from 0.1 to 1.9
- routes: int32 [1024, 2], P('ep'), may hold values from 0 to 7, all different within a row; in each aligned block of 128 rows (0 to 127, 128 to 255, ...) at most 64 rows name the same one
- route_weight: float32 [1024, 2], P('ep'), may hold values from 0.1 to 2.5
- expert_switch_matrix: bfloat16 [8, 2048, 4096], P('ep', None, 'tp'), may hold values from -0.125 to 0.125
- up_weight: bfloat16 [8, 2048, 4096], P('ep', None, 'tp'), may hold values from -0.125 to 0.125
- down_weight: bfloat16 [8, 4096, 2048], P('ep', None, 'tp'), may hold values from -0.09375 to 0.09375
- shared_gate: bfloat16 [2048, 1024], P(None, 'tp'), may hold values from -0.125 to 0.125
- shared_up: bfloat16 [2048, 1024], P(None, 'tp'), may hold values from -0.125 to 0.125
- shared_down: bfloat16 [1024, 2048], P(None, 'tp'), may hold values from -0.1875 to 0.1875
Outputs:
- mixer_out: bfloat16 [2048, 2048], P('ep', 'tp')
- experts_out: bfloat16 [1024, 2048], P('ep', 'tp')
The draws below stay inside these ranges and needn't reach their ends.
Inputs may be any that keep to these rules, and one draw needn't show every extreme that they name: `routes`: each row names 2 different experts. In each aligned block of 128 rows (the rows of one index of ep) no expert is named by more than 64 rows, and in some block one expert is named by exactly 64 rows.
All inputs are finite; a program needn't handle non-finite values.
Results may differ from the reference program's by a relative error of at most 0.0069.
Values may be sent and summed in bfloat16 or wider, within the bound.
A program may use at most 128 MiB of HBM per device.

```python
import math
import jax
import jax.numpy as jnp
import numpy as np
from jax import lax

D = 2048
GROUPS = 64
GROUP = 16
STATE = 64
EXPERT_FF = 4096
FF = 1024
TOPK = 2
MIX_ROWS = 256
EXP_ROWS = 128
D_SSM = 1024
MIX_TOKENS = 2048
EXP_TOKENS = 1024
EXPERTS = 8
CAP = 64
N_EP = 8


def draw_steps(key):
    pick_key, fast_key, slow_key = jax.random.split(key, 3)
    quick = jax.random.randint(pick_key, (GROUPS,), 0, 2) < 1
    fast = jax.random.uniform(fast_key, (GROUPS,), jnp.float32, math.log(0.02), math.log(0.067))
    slow = jax.random.uniform(slow_key, (GROUPS,), jnp.float32, math.log(0.2), math.log(1.2)) - math.log(MIX_TOKENS)
    return jnp.where(quick, fast, slow)


def draw_log_step(key, part):
    return draw_steps(jax.random.fold_in(key, 101))


def draw_input_map(key, part):
    steps = draw_steps(jax.random.fold_in(key, 101))
    noise_key = jax.random.fold_in(key, 202)
    noise = jax.random.truncated_normal(noise_key, -4.0, 4.0, (2, GROUPS, STATE, GROUP), jnp.float32)
    scale = jnp.exp(-0.5 * steps)[None, :, None, None] / math.sqrt(2.0 * GROUP)
    return (noise * scale).astype(jnp.bfloat16)


def draw_decay_shift(key, part):
    rate_key, place_key, depth_key = jax.random.split(jax.random.fold_in(key, 303), 3)
    block_count = MIX_TOKENS // MIX_ROWS
    lowest, highest = (0.05, 0.4)
    block_rate = jnp.exp(jax.random.uniform(rate_key, (block_count, GROUPS), jnp.float32, math.log(lowest), math.log(highest))) / MIX_TOKENS
    shift_magnitude = -jnp.repeat(block_rate, MIX_ROWS, axis=0)
    capacity_indices = jax.random.randint(place_key, (2, GROUPS), 0, MIX_TOKENS)
    stack_levels = jnp.log(jax.random.uniform(depth_key, (2, GROUPS), jnp.float32, 0.55, 0.8))
    element_ordinals = jnp.arange(MIX_TOKENS, dtype=jnp.int32)[:, None, None]
    sequence_groupings = jnp.sum(jnp.where(element_ordinals == capacity_indices[None], stack_levels[None], 0.0), axis=1)
    return shift_magnitude + sequence_groupings


def steps_of(key, shape, pieces, least, high):
    def one(axis_at, blocks):
        steps = jax.random.uniform(jax.random.fold_in(jax.random.fold_in(key, 6), axis_at), (blocks,), jnp.float32, least / len(pieces), high / len(pieces))
        return jnp.repeat(jnp.exp(steps), shape[axis_at] // blocks).reshape((-1,) + (1,) * (len(shape) - axis_at - 1))

    level = one(*pieces[0])
    for cut in pieces[1:]:
        level = level * one(*cut)
    return level


def routed_block(key, own, number, rows, count, top, reach, slope):
    sequence = jax.random.permutation(key, count)
    crowded, common = load_shares(count, rows * top, reach, slope, True), load_shares(count, rows * top, reach, slope, False)
    places = jnp.arange(count)

    def named(tallies, turn):
        used = int((tallies > 0).sum())
        fixed = max(1, used // 4)
        shifted = fixed + (places - fixed + turn * (used - fixed)) % max(1, count - fixed)
        return jnp.zeros((count,), jnp.int32).at[sequence[jnp.where(places < fixed, places, shifted)]].set(jnp.asarray(tallies, jnp.int32))

    tallies = jnp.where(number % 4 == 0, named(crowded, number // 4), named(common, number - number // 4 - 1))
    mixed = jax.random.permutation(jax.random.fold_in(own, 3), count)
    donor, receiver = mixed[0:count // 2 * 2:2], mixed[1:count // 2 * 2:2]
    room = jnp.minimum(tallies[donor] - 1, reach - tallies[receiver]) // 2
    room = jnp.where((donor == sequence[0]) | (receiver == sequence[0]) | (tallies[receiver] == 0), 0, jnp.maximum(room, 0))
    shifted = jax.random.randint(jax.random.fold_in(own, 4), (count // 2,), 0, 1 << 20) % (room + 1)
    tallies = tallies.at[donor].add(-shifted).at[receiver].add(shifted)
    items = jnp.searchsorted(jnp.cumsum(tallies), jnp.arange(rows * top), side="right").astype(jnp.int32)
    table = items.reshape(top, rows).T
    table = table[jax.random.permutation(jax.random.fold_in(own, 1), rows)]
    turn = jax.random.randint(jax.random.fold_in(own, 2), (rows, 1), 0, top)
    return jnp.take_along_axis(table, (jnp.arange(top)[None, :] + turn) % top, axis=1)


def load_shares(amount, total, most, lean, full):
    weights = [(1 << 20) // math.isqrt(rank ** lean) + 1 for rank in range(1, amount + 1)]
    largest = most if full else min(most, max(-(-total // amount), total * weights[0] // sum(weights)))
    least = 1 if total - largest >= amount - 1 else 0
    holding, surplus = [largest] + [least] * (amount - 1), total - largest - least * (amount - 1)
    while surplus > 0:
        free = [i for i in range(1, amount) if holding[i] < largest] or [i for i in range(1, amount) if holding[i] < most]
        pool, remaining = sum([weights[i] for i in free]), surplus
        for i in free:
            addition = min(most - holding[i], max(1, remaining * weights[i] // pool), surplus)
            holding[i] = holding[i] + addition
            surplus = surplus - addition
    return np.array(holding)


def normal_values(key, shape, scale, bound, cuts=(), held_as=jnp.bfloat16):
    drawn = jax.random.normal(key, shape, jnp.float32) * scale
    if len(cuts) > 0:
        drawn = steps_of(key, shape, cuts, -0.22, 0.18) * drawn
    return jnp.clip(drawn, min=-bound, max=bound).astype(held_as)


def setup_inputs(seed: int = 0) -> dict:
    arg_keys = jax.random.split(jax.random.key(seed), 17)
    mixer_input = normal_values(arg_keys[0], (MIX_TOKENS, D_SSM), 1.0, 6.0, ((0, 8), (1, 4)))
    log_step = draw_log_step(jax.random.fold_in(arg_keys[16], 71), 0)
    decay_shift = draw_decay_shift(jax.random.fold_in(arg_keys[16], 71), 0)
    input_map = draw_input_map(jax.random.fold_in(arg_keys[16], 71), 0)
    readout = normal_values(arg_keys[4], (2, GROUPS, GROUP, STATE), (2 * STATE) ** -0.5, 0.5, ((1, 4),), jnp.float32)
    mixer_weight = normal_values(arg_keys[5], (D_SSM, D), D_SSM ** -0.5, 0.1875, ((1, 4),))
    expert_input = normal_values(arg_keys[6], (EXP_TOKENS, D), 1.0, 6.0, ((0, 8),))
    norm_gain = jnp.clip(1.0 + 0.18 * jax.random.normal(arg_keys[7], (D,), jnp.float32), 0.1, 1.9)
    routes_keys = jax.random.split(jax.random.fold_in(arg_keys[8], 1), EXP_TOKENS // EXP_ROWS)
    routes_turns = jax.random.permutation(jax.random.fold_in(arg_keys[8], 3), EXP_TOKENS // EXP_ROWS)
    routes = jax.vmap(lambda own, number: routed_block(jax.random.fold_in(arg_keys[8], 2), own, number, EXP_ROWS, EXPERTS, TOPK, CAP, 1))(routes_keys, routes_turns).reshape((EXP_TOKENS, TOPK))
    route_weight = jnp.clip(jnp.exp(math.log(2.5) - 3.218876 * jax.random.uniform(arg_keys[9], (EXP_TOKENS, TOPK), jnp.float32) ** steps_of(arg_keys[9], (EXP_TOKENS, TOPK), ((0, 8),), -0.2, 0.2)), 0.1, 2.5)
    expert_switch_matrix = normal_values(arg_keys[10], (EXPERTS, D, EXPERT_FF), D ** -0.5, 0.125, ((0, 8), (2, 4)))
    up_weight = normal_values(arg_keys[11], (EXPERTS, D, EXPERT_FF), D ** -0.5, 0.125, ((0, 8), (2, 4)))
    down_weight = normal_values(arg_keys[12], (EXPERTS, EXPERT_FF, D), EXPERT_FF ** -0.5, 0.09375, ((0, 8), (2, 4)))
    shared_gate = normal_values(arg_keys[13], (D, FF), D ** -0.5, 0.125, ((1, 4),))
    shared_up = normal_values(arg_keys[14], (D, FF), D ** -0.5, 0.125, ((1, 4),))
    shared_down = normal_values(arg_keys[15], (FF, D), FF ** -0.5, 0.1875, ((1, 4),))
    return {"mixer_input": mixer_input, "log_step": log_step, "decay_shift": decay_shift, "input_map": input_map, "readout": readout, "mixer_weight": mixer_weight, "expert_input": expert_input, "norm_gain": norm_gain, "routes": routes, "route_weight": route_weight, "expert_switch_matrix": expert_switch_matrix, "up_weight": up_weight, "down_weight": down_weight, "shared_gate": shared_gate, "shared_up": shared_up, "shared_down": shared_down}


def combine_parts(earlier, later):
    early_real, early_imaginary, early_shift_real, early_shift_imaginary = earlier
    late_real, late_imaginary, late_shift_real, late_shift_imaginary = later
    joint_real = late_real * early_real - late_imaginary * early_imaginary
    joint_imaginary = late_real * early_imaginary + late_imaginary * early_real
    shift_real = late_real * early_shift_real - late_imaginary * early_shift_imaginary + late_shift_real
    shift_imaginary = late_real * early_shift_imaginary + late_imaginary * early_shift_real + late_shift_imaginary
    return (joint_real, joint_imaginary, shift_real, shift_imaginary)

def factors(log_step, states):
    step_rate = jnp.exp(log_step)
    frequency = jnp.pi * jnp.arange(states, dtype=jnp.float32)
    angle = step_rate[:, None] * frequency[None, :]
    turn_cosine = jnp.cos(angle)
    turn_sine = jnp.sin(angle)
    base = jnp.exp(-0.5 * step_rate)[:, None]
    base_real = base * turn_cosine
    starting_quadrature = base * turn_sine
    inverse = 1.0 / (0.25 + frequency * frequency)[None, :]
    lowered = base_real - 1.0
    inject_real = (-0.5 * lowered + starting_quadrature * frequency[None, :]) * inverse
    inject_imaginary = (-0.5 * starting_quadrature - lowered * frequency[None, :]) * inverse
    return (step_rate, turn_cosine, turn_sine, inject_real, inject_imaginary)

def reference(mixer_input, log_step, decay_shift, input_map, readout, mixer_weight, expert_input, norm_gain, routes, route_weight, expert_switch_matrix, up_weight, down_weight, shared_gate, shared_up, shared_down):
    highest = lax.Precision.HIGHEST
    step_rate, turn_cosine, turn_sine, inject_real, inject_imaginary = factors(log_step, STATE)
    blocks_in = mixer_input.reshape(N_EP, MIX_ROWS, GROUPS, GROUP)
    blocks_shift = decay_shift.reshape(N_EP, MIX_ROWS, GROUPS)
    map_real = input_map[0].astype(jnp.float32)
    map_imaginary = input_map[1].astype(jnp.float32)

    def advance(carry, inputs):
        carry_real, carry_imaginary = carry
        block_in, block_shift = inputs
        magnitude = jnp.exp(-0.5 * step_rate[None, :] + block_shift)[:, :, None]
        decay_real = magnitude * turn_cosine[None]
        decay_imaginary = magnitude * turn_sine[None]
        values = block_in.astype(jnp.float32)
        drive_real = jnp.einsum('tgh,gph->tgp', values, map_real, precision=highest)
        drive_imaginary = jnp.einsum('tgh,gph->tgp', values, map_imaginary, precision=highest)
        push_real = inject_real[None] * drive_real - inject_imaginary[None] * drive_imaginary
        push_imaginary = inject_real[None] * drive_imaginary + inject_imaginary[None] * drive_real
        total_real, total_imaginary, local_real, local_imaginary = lax.associative_scan(combine_parts, (decay_real, decay_imaginary, push_real, push_imaginary), axis=0)
        state_real = local_real + total_real * carry_real[None] - total_imaginary * carry_imaginary[None]
        state_imaginary = local_imaginary + total_real * carry_imaginary[None] + total_imaginary * carry_real[None]
        mixed = jnp.einsum('ghp,tgp->tgh', readout[0], state_real, precision=highest) - jnp.einsum('ghp,tgp->tgh', readout[1], state_imaginary, precision=highest)
        return ((state_real[-1], state_imaginary[-1]), mixed.reshape(MIX_ROWS, GROUPS * GROUP))
    start = (jnp.zeros((GROUPS, STATE), jnp.float32), jnp.zeros((GROUPS, STATE), jnp.float32))
    _, outputs = lax.scan(advance, start, (blocks_in, blocks_shift))
    activated = jax.nn.gelu(outputs.reshape(MIX_TOKENS, GROUPS * GROUP)).astype(jnp.bfloat16)
    mixer_out = jnp.dot(activated, mixer_weight, preferred_element_type=jnp.float32).astype(jnp.bfloat16)
    values = expert_input.astype(jnp.float32)
    normed = (values * lax.rsqrt(lax.optimization_barrier(jnp.mean(values * values, axis=-1, keepdims=True)) + 1e-06) * norm_gain).astype(jnp.bfloat16)
    shared_hidden = (jax.nn.silu(jnp.dot(normed, shared_gate, preferred_element_type=jnp.float32)) * jnp.dot(normed, shared_up, preferred_element_type=jnp.float32)).astype(jnp.bfloat16)
    common_contribution = jnp.dot(shared_hidden, shared_down, preferred_element_type=jnp.float32)
    token_count = EXP_TOKENS
    limit = N_EP * CAP
    padded = jnp.concatenate([normed, jnp.zeros((1, D), jnp.bfloat16)], axis=0)

    def expert_step(total, expert):
        chosen = routes == expert
        member = jnp.any(chosen, axis=1)
        weight = lax.optimization_barrier(jnp.sum(jnp.where(chosen, route_weight, 0.0), axis=1))
        position = (jnp.cumsum(member.astype(jnp.int32)) - 1).astype(jnp.int32)
        target = jnp.where(member, position, limit).astype(jnp.int32)
        holder = jnp.full((limit,), token_count, jnp.int32).at[target].set(jnp.arange(token_count, dtype=jnp.int32), mode='drop')
        rows = padded[holder]
        hidden = (jax.nn.silu(jnp.dot(rows, expert_switch_matrix[expert], preferred_element_type=jnp.float32)) * jnp.dot(rows, up_weight[expert], preferred_element_type=jnp.float32)).astype(jnp.bfloat16)
        part = jnp.dot(hidden, down_weight[expert], preferred_element_type=jnp.float32).astype(jnp.bfloat16)
        scale = jnp.concatenate([weight, jnp.zeros((1,), jnp.float32)], axis=0)[holder]
        return (total.at[holder].add(part.astype(jnp.float32) * scale[:, None]), None)
    routed_output, _ = lax.scan(expert_step, jnp.zeros((token_count + 1, D), jnp.float32), jnp.arange(EXPERTS, dtype=jnp.int32))
    experts_out = (common_contribution + routed_output[:token_count]).astype(jnp.bfloat16)
    return (mixer_out, experts_out)
```

```python
import functools
import math

import jax
import jax.numpy as jnp
from jax import lax
from jax.experimental import pallas as pl
from jax.experimental.pallas import tpu as pltpu
from jax.sharding import PartitionSpec as P

MESH = pl.DeviceIdType.MESH
SUBLANES = 8
NT = (((1,), (1,)), ((), ()))
TN = (((0,), (0,)), ((), ()))


def times(ar, ai, br, bi):
    return ar * br - ai * bi, ar * bi + ai * br


def iota(shape, dim):
    return lax.broadcasted_iota(jnp.int32, shape, dim)


def spread(shape, period):
    return (iota(shape, 1) % period == iota(shape, 0)).astype(jnp.bfloat16)


def halves(a):
    high = a.astype(jnp.bfloat16)
    return high, (a - high.astype(jnp.float32)).astype(jnp.bfloat16)


def dot(a, b, dims=None):
    if dims is None:
        return jnp.dot(a, b, preferred_element_type=jnp.float32)
    return lax.dot_general(a, b, dims, preferred_element_type=jnp.float32)


def fill_table(rate_ref, table, states):
    groups = rate_ref.shape[1]
    merged = table.shape[1]
    same = iota((groups, groups), 0) == iota((groups, groups), 1)
    column = jnp.sum(jnp.where(same, rate_ref[...], 0.0), axis=1, keepdims=True)
    place = iota((groups, merged), 1) // states == iota((groups, merged), 0)
    wide = jnp.sum(jnp.where(place, column, 0.0), axis=0, keepdims=True)
    step_rate = jnp.exp(wide)
    frequency = jnp.pi * lax.rem(iota((1, merged), 1), states).astype(jnp.float32)
    angle = step_rate * frequency
    turn_cosine = jnp.cos(angle)
    turn_sine = jnp.sin(angle)
    base = jnp.exp(-0.5 * step_rate)
    starting_quadrature = base * turn_sine
    inverse = 1.0 / (0.25 + frequency * frequency)
    lowered = base * turn_cosine - 1.0
    table[0:1, :] = turn_cosine
    table[1:2, :] = turn_sine
    table[2:3, :] = (-0.5 * lowered + starting_quadrature * frequency) * inverse
    table[3:4, :] = (-0.5 * starting_quadrature - lowered * frequency) * inverse
    return column


def drive_into(x_ref, column, shift_ref, map_ref, table_ref, mag, push_re, push_im, states):
    rows, channels = x_ref.shape
    merged = mag.shape[1]
    groups = shift_ref.shape[0]
    width = channels // groups
    steps = rows // SUBLANES
    place = iota((rows, rows), 0)
    order = (iota((rows, rows), 1) == (place % SUBLANES) * steps + place // SUBLANES).astype(
        jnp.bfloat16
    )
    level = jnp.exp(-0.5 * jnp.exp(column) + shift_ref[...])
    high, middle = halves(level)
    low = ((level - high.astype(jnp.float32)) - middle.astype(jnp.float32)).astype(jnp.bfloat16)
    widen = (iota((groups, merged), 1) // states == iota((groups, merged), 0)).astype(jnp.bfloat16)
    total = None
    for piece in (high, middle, low):
        part = dot(dot(order, piece, NT).astype(jnp.bfloat16), widen)
        total = part if total is None else total + part
    mag[...] = total
    x = dot(order, x_ref[...]).astype(jnp.bfloat16)
    repeat = spread((states, merged), states)
    mine = iota((channels, merged), 1) // states == iota((channels, merged), 0) // width
    drives = []
    for c in range(2):
        wide = jnp.where(mine, dot(map_ref[c], repeat), 0.0).astype(jnp.bfloat16)
        drives.append(dot(x, wide))
    re, im = times(table_ref[2:3, :], table_ref[3:4, :], drives[0], drives[1])
    push_re[...] = re
    push_im[...] = im


def sweep(table_ref, mag, push_re, push_im, start_re, start_im, keep):
    rows, merged = mag.shape
    turn_re = jnp.broadcast_to(table_ref[0:1, :], (SUBLANES, merged))
    turn_im = jnp.broadcast_to(table_ref[1:2, :], (SUBLANES, merged))

    def one(j, carry):
        re, im, product = carry
        at = pl.ds(pl.multiple_of(j * SUBLANES, SUBLANES), SUBLANES)
        level = mag[at, :]
        next_re, next_im = times(turn_re, turn_im, re, im)
        next_re = level * next_re + push_re[at, :]
        next_im = level * next_im + push_im[at, :]
        if keep:
            push_re[at, :] = next_re
            push_im[at, :] = next_im
        else:
            product = product * level
        return next_re, next_im, product

    product = jnp.ones((SUBLANES, merged), jnp.float32)
    if keep:
        def pair(j, carry):
            return one(j, carry + (None,))[:2]
        return lax.fori_loop(0, rows // SUBLANES, pair, (start_re, start_im))
    return lax.fori_loop(0, rows // SUBLANES, one, (start_re, start_im, product))


def join(table_ref, ends_re, ends_im, product, pre, steps):
    merged = ends_re.shape[1]
    wr, wi = table_ref[0:1, :], table_ref[1:2, :]
    power = 1
    while power < steps:
        wr, wi = times(wr, wi, wr, wi)
        power *= 2
    cr = jnp.zeros((1, merged), jnp.float32)
    ci = cr
    ar = cr + 1.0
    ai = cr
    for s in range(SUBLANES):
        for i, v in enumerate((cr, ci, ar, ai)):
            pre[i, s : s + 1, :] = v
        level = product[s : s + 1]
        fr, fi = level * wr, level * wi
        tr, ti = times(fr, fi, cr, ci)
        cr, ci = tr + ends_re[s : s + 1], ti + ends_im[s : s + 1]
        ar, ai = times(fr, fi, ar, ai)
    return cr, ci, ar, ai


def read_states(readout_ref, push_re, push_im, states):
    rows, merged = push_re.shape
    channels = readout_ref.shape[1]
    width = channels * states // merged
    repeat = spread((states, merged), states)
    mine = iota((channels, merged), 1) // states == iota((channels, merged), 0) // width
    total = None
    for c, ref in enumerate((push_re, push_im)):
        high, low = halves(ref[...])
        back = readout_ref[c] if c == 0 else -readout_ref[c]
        wide_high, wide_low = (
            jnp.where(mine, dot(half, repeat), 0.0).astype(jnp.bfloat16) for half in halves(back)
        )
        part = dot(high, wide_high, NT) + (dot(low, wide_high, NT) + dot(high, wide_low, NT))
        total = part if total is None else total + part
    place = iota((rows, rows), 0)
    steps = rows // SUBLANES
    order = (iota((rows, rows), 1) == (place % steps) * SUBLANES + place // steps).astype(
        jnp.bfloat16
    )
    cube = total + 0.044715 * (total * total * total)
    active = (0.5 * total * (1.0 + jnp.tanh(0.7978845608028654 * cube))).astype(jnp.bfloat16)
    return dot(order, active).astype(jnp.bfloat16)


def remote(src, dst, send, recv, **target):
    return pltpu.make_async_remote_copy(
        src_ref=src, dst_ref=dst, send_sem=send, recv_sem=recv,
        device_id=target, device_id_type=MESH,
    )


def visits(chips):
    plan = []
    for chip in range(chips):
        units = []
        for d in range(1, chips):
            for j in range(2):
                together = False
                for there, onward in ((chip - d, chip + 1), (chip + d, chip - 1)):
                    if 0 <= there < chips:
                        onward = onward if 0 <= onward < chips else -1
                        units.append((2 * there + j, onward, int(together)))
                        together = True
        plan.append(units)
    return plan


def fused_kernel(
    n_ep, n_tp, states,
    routes_ref, gains_ref, rate_ref, gain_ref,
    input_hbm, x_hbm, shift_hbm, map_hbm, readout_hbm, weight_hbm,
    sgate_hbm, sup_hbm, sdown_hbm, gate_hbm, up_hbm, down_hbm,
    out_ref, experts_ref,
    tokens, x_ref, shift_ref, map_ref, readout_ref, weight_ref,
    sgate, sup, sdown, gate, up, down,
    table, mag, push_re, push_im, pre, summary, active,
    tok, named, picked, hidden, result, returned, shared, common, high, low,
    load, tok_recv, mate_send, own_send, on_send, n_send, n_recv,
    e_send, e_recv, a_send, a_recv, h_send, h_recv, r_send, r_recv, s_send, s_recv,
):
    ep = lax.axis_index("ep")
    tp = lax.axis_index("tp")
    rows, channels = x_ref.shape
    merged = mag.shape[1]
    half_rows, features = tok.shape[2:]
    count = 2 * half_rows
    cap = picked.shape[0]
    chips = n_ep // 2
    chip, core = ep // 2, lax.rem(ep, 2)
    mate = ep + 1 - 2 * core
    side = math.isqrt(n_tp)
    y, x = tp // side, lax.rem(tp, side)
    half = hidden.shape[4]

    barrier = pltpu.get_barrier_semaphore()
    for d in range(1, n_ep):
        pl.semaphore_signal(
            barrier, inc=1, device_id={"ep": lax.rem(ep + d, n_ep)}, device_id_type=MESH
        )
    for d in range(1, n_tp):
        pl.semaphore_signal(
            barrier, inc=1, device_id={"tp": lax.rem(tp + d, n_tp)}, device_id_type=MESH
        )
    pairs = (
        (input_hbm, tokens), (sgate_hbm, sgate), (sup_hbm, sup), (gate_hbm, gate), (up_hbm, up),
        (x_hbm, x_ref), (shift_hbm, shift_ref), (map_hbm, map_ref), (down_hbm, down),
        (readout_hbm, readout_ref), (weight_hbm, weight_ref), (sdown_hbm, sdown),
    )
    loads = [pltpu.make_async_copy(a, b, load.at[i]) for i, (a, b) in enumerate(pairs)]
    for copy in loads:
        copy.start()
    sends = []

    def go(copy):
        copy.start()
        sends.append(copy)

    def across(dy, dx):
        return lax.rem(y + dy, side) * side + lax.rem(x + dx, side)

    peers = {(dy, dx): across(dy, dx) for dy in range(side) for dx in range(side)}

    class Share:
        def __init__(self, at, send, recv):
            self.at, self.send, self.recv = at, send, recv

        def copy(self, source, h, dy, dx, to):
            return remote(
                self.at(source, h), self.at(source, h), self.send(h, dy, dx),
                self.recv(source, h), tp=to,
            )

        def start(self, h):
            for o in range(1, side):
                go(self.copy(tp, h, 0, o, peers[0, o]))
                go(self.copy(tp, h, o, 0, peers[o, 0]))

        def wait(self, source, h):
            self.copy(source, h, 0, 0, source).wait_recv()

        def forward(self):
            for o in range(1, side):
                self.wait(peers[0, o], 0)
                for d in range(1, side):
                    go(self.copy(peers[0, o], 0, d, o, peers[d, 0]))
                self.wait(peers[o, 0], 1)
                for d in range(1, side):
                    go(self.copy(peers[o, 0], 1, o, d, peers[0, d]))

        def near(self):
            for o in range(1, side):
                self.wait(peers[0, o], 1)
                self.wait(peers[o, 0], 0)

        def far(self):
            for dy in range(1, side):
                for dx in range(1, side):
                    for h in range(2):
                        self.wait(peers[dy, dx], h)

    def hidden_of(s):
        return Share(
            lambda q, h: hidden.at[s, q, h],
            lambda h, dy, dx: h_send.at[s, h, dy * side + dx],
            lambda q, h: h_recv.at[s, q, h],
        )

    shared_out = Share(
        lambda q, h: shared.at[q, h],
        lambda h, dy, dx: s_send.at[h, dy * side + dx],
        lambda q, h: s_recv.at[q, h],
    )
    active_out = Share(
        lambda q, h: active.at[q, h],
        lambda h, dy, dx: a_send.at[h, dy * side + dx],
        lambda q, h: a_recv.at[q, h],
    )

    loads[0].wait()
    block = 16
    scale = gain_ref[...]

    @pl.loop(0, half_rows // block)
    def _(i):
        at = pl.ds(pl.multiple_of(i * block, block), block)
        for h in range(2):
            values = tokens[h, at, :].astype(jnp.float32)
            level = lax.rsqrt(jnp.mean(values * values, axis=-1, keepdims=True) + 1e-06)
            tok[ep, h, at, :] = (values * level * scale).astype(jnp.bfloat16)

    named[ep] = routes_ref[...]
    pl.semaphore_wait(barrier, n_ep + n_tp - 2)

    def piece(s, h, send, target):
        return remote(tok.at[s, h], tok.at[s, h], send, tok_recv.at[s, h], ep=target)

    go(piece(ep, 1 - core, mate_send.at[ep, 1 - core], mate))
    go(piece(ep, core, mate_send.at[ep, core], mate))
    for d in range(1, n_ep):
        target = lax.rem(ep + d, n_ep)
        go(remote(routes_ref, named.at[ep], n_send.at[d], n_recv.at[ep], ep=target))
    ends = ((chip > 0, lax.rem(ep + n_ep - 2, n_ep)), (chip < chips - 1, lax.rem(ep + 2, n_ep)))

    def own(j, d):
        return piece(2 * chip + j, core, own_send.at[d, j], ends[d][1])

    for j in range(2):
        @pl.when(core != j)
        def _():
            piece(2 * chip + j, core, mate_send.at[mate, core], mate).wait_recv()

        for d in range(2):
            @pl.when(ends[d][0])
            def _():
                own(j, d).start()

    def shared_hidden():
        for copy in loads[1:3]:
            copy.wait()
        a = tok[ep].reshape(count, features)
        v = dot(a, sgate[...])
        shared[tp] = (v / (1.0 + jnp.exp(-v)) * dot(a, sup[...])).astype(jnp.bfloat16).reshape(
            shared.shape[1:]
        )
        for h in range(2):
            shared_out.start(h)

    later = (iota((count, count), 0) <= iota((count, count), 1)).astype(jnp.bfloat16)
    slots = iota((cap, count), 0).astype(jnp.float32)

    def member(names, expert):
        return jnp.logical_or(names[0:1] == expert, names[1:2] == expert)

    def seats(mine):
        ones = jnp.where(mine, 1.0, 0.0)
        ranks = dot(ones.astype(jnp.bfloat16), later)
        return jnp.where(mine, ranks - 1.0, -1.0)

    tile = min(half, 256)

    def process(s):
        names = named[s]
        place = seats(jnp.broadcast_to(member(names, ep), (SUBLANES, count)))
        chosen = (slots == place[0:1]).astype(jnp.bfloat16)
        picked[...] = dot(chosen, tok[s].reshape(count, features)).astype(jnp.bfloat16)
        share = hidden_of(s)
        for h in range(2):
            @pl.loop(0, half // tile)
            def _(n):
                inner = pl.ds(pl.multiple_of(n * tile, tile), tile)
                at = pl.ds(pl.multiple_of(h * half + n * tile, tile), tile)
                a = picked[...]
                v = dot(a, gate[:, at])
                hidden[s, tp, h, :, inner] = (
                    v / (1.0 + jnp.exp(-v)) * dot(a, up[:, at])
                ).astype(jnp.bfloat16)

            share.start(h)

    def back(s):
        return remote(result.at[s], returned.at[ep], r_send.at[s], r_recv.at[ep], ep=s)

    def project(s, away=True):
        share = hidden_of(s)

        def part(q):
            return dot(hidden[s, q, 0], down[q, 0]) + dot(hidden[s, q, 1], down[q, 1])

        share.near()
        total = part(tp)
        for o in range(1, side):
            total = total + part(peers[0, o])
            total = total + part(peers[o, 0])
        share.far()
        for dy in range(1, side):
            for dx in range(1, side):
                total = total + part(peers[dy, dx])
        if away:
            result[s] = total.astype(jnp.bfloat16)
            go(back(s))
        else:
            returned[s] = total.astype(jnp.bfloat16)

    def scan_block():
        for copy in loads[5:8]:
            copy.wait()
        column = fill_table(rate_ref, table, states)
        drive_into(x_ref, column, shift_ref, map_ref, table, mag, push_re, push_im, states)
        zero = jnp.zeros((SUBLANES, merged), jnp.float32)
        ends_re, ends_im, product = sweep(table, mag, push_re, push_im, zero, zero, False)
        end = join(table, ends_re, ends_im, product, pre, rows // SUBLANES)
        for i, v in enumerate(end):
            summary[ep, i : i + 1, :] = v
        for d in range(1, n_ep):
            go(remote(
                summary.at[ep], summary.at[ep], e_send.at[d], e_recv.at[ep],
                ep=lax.rem(ep + d, n_ep),
            ))

    def gain_blocks():
        names = routes_ref[...]
        level = gains_ref[...]
        for e in range(n_ep):
            place = seats(jnp.broadcast_to(member(names, e), (SUBLANES, count)))
            weight = jnp.where(names[0:1] == e, level[0:1], 0.0) + jnp.where(
                names[1:2] == e, level[1:2], 0.0
            )
            wide = jnp.where(slots == place[0:1], weight, 0.0)
            top, rest = halves(wide)
            high[e * cap : (e + 1) * cap, :] = top
            low[e * cap : (e + 1) * cap, :] = rest

    def scan_states():
        for d in range(1, n_ep):
            e = lax.rem(ep + d, n_ep)
            remote(
                summary.at[e], summary.at[e], e_send.at[d], e_recv.at[e], ep=e
            ).wait_recv()

        def fold(e, carry):
            part = summary[e]
            re, im = times(part[2:3], part[3:4], carry[0], carry[1])
            return re + part[0:1], im + part[1:2]

        nothing = jnp.zeros((1, merged), jnp.float32)
        in_re, in_im = lax.fori_loop(0, ep, fold, (nothing, nothing))
        add_re, add_im = times(pre[2], pre[3], in_re, in_im)
        sweep(table, mag, push_re, push_im, pre[0] + add_re, pre[1] + add_im, True)
        loads[9].wait()
        active[tp] = read_states(readout_ref, push_re, push_im, states).reshape(active.shape[1:])
        for h in range(2):
            active_out.start(h)

    def mix():
        active_out.near()
        active_out.far()
        loads[10].wait()
        total = None
        for q in range(n_tp):
            a = active[q].reshape(rows, channels)
            part = dot(a, weight_ref[q * channels : (q + 1) * channels, :])
            total = part if total is None else total + part
        out_ref[...] = total.astype(out_ref.dtype)
        shared_out.near()
        shared_out.far()
        loads[11].wait()
        width = shared.shape[3]
        total = None
        for q in range(n_tp):
            a = shared[q].reshape(count, width)
            part = dot(a, sdown[q * width : (q + 1) * width, :])
            total = part if total is None else total + part
        common[...] = total

    plan = visits(chips)
    last = len(plan[0]) - 1

    def here(u, field):
        value = jnp.int32(plan[0][u][field])
        for k in range(1, chips):
            value = jnp.where(chip == k, jnp.int32(plan[k][u][field]), value)
        return value

    source = [here(u, 0) for u in range(last + 1)]
    onward = [here(u, 1) for u in range(last + 1)]
    paired = [here(u, 2) for u in range(last + 1)]

    def along(u):
        target = 2 * jnp.maximum(onward[u], 0) + core
        return piece(source[u], core, on_send.at[source[u]], target)

    def aside(u):
        return piece(source[u], core, mate_send.at[source[u], core], mate)

    def pass_on(u):
        aside(u).wait_recv()

        @pl.when(onward[u] >= 0)
        def _():
            along(u).start()

        aside(u).start()

    shared_hidden()
    for copy in loads[3:5]:
        copy.wait()
    process(ep)
    piece(mate, 1 - core, mate_send.at[mate, 1 - core], mate).wait_recv()

    def names_of(s):
        remote(routes_ref, named.at[s], n_send.at[0], n_recv.at[s], ep=s).wait_recv()

    names_of(mate)
    process(mate)
    scan_block()
    gain_blocks()
    shared_out.forward()
    order = [ep, mate] + source
    for u in range(last + 1):
        @pl.when(paired[u] == 0)
        def _():
            pass_on(u)

        if u < last:
            @pl.when(paired[u + 1] == 1)
            def _():
                pass_on(u + 1)

        if u == 0:
            hidden_of(ep).forward()
        hidden_of(order[u + 1]).forward()
        s = source[u]
        piece(s, 1 - core, mate_send.at[s, 1 - core], mate).wait_recv()
        names_of(s)
        process(s)
        if u == 0:
            loads[8].wait()
        project(order[u], away=u > 0)
        if u == min(2, last):
            scan_states()
        if u == min(3, last):
            active_out.forward()
        if u == min(4, last):
            mix()
    hidden_of(order[-1]).forward()
    project(order[-2])
    project(order[-1])
    for d in range(1, n_ep):
        e = lax.rem(ep + d, n_ep)
        remote(returned.at[e], returned.at[e], r_send.at[e], r_recv.at[e], ep=e).wait_recv()
    back_rows = returned[...].reshape(n_ep * cap, returned.shape[2])
    routed = dot(high[...], back_rows, TN) + dot(low[...], back_rows, TN)
    experts_ref[...] = (common[...] + routed).astype(experts_ref.dtype)
    for copy in sends:
        copy.wait_send()
    for j in range(2):
        for d in range(2):
            @pl.when(ends[d][0])
            def _():
                own(j, d).wait_send()
    for u in range(last + 1):
        aside(u).wait_send()

        @pl.when(onward[u] >= 0)
        def _():
            along(u).wait_send()


def shards(
    mixer_input,
    log_step,
    decay_shift,
    input_map,
    readout,
    mixer_weight,
    expert_input,
    norm_gain,
    routes,
    route_weight,
    expert_switch_matrix,
    up_weight,
    down_weight,
    shared_gate,
    shared_up,
    shared_down,
):
    n_ep, n_tp = lax.axis_size("ep"), lax.axis_size("tp")
    count, features = expert_input.shape
    cap = 2 * count * routes.shape[1] // n_ep
    rows, channels = mixer_input.shape
    groups = log_step.shape[0]
    states, width = input_map.shape[2:]
    merged = groups * states
    f32, bf16 = jnp.float32, jnp.bfloat16
    ff = up_weight.shape[2]
    depth, columns = down_weight.shape[1:]
    shared_ff = shared_up.shape[1]
    vmem = pl.BlockSpec(memory_space=pltpu.VMEM)
    anywhere = pl.BlockSpec(memory_space=pl.ANY)
    dma = pltpu.SemaphoreType.DMA
    operands = (
        expert_input.reshape(2, count // 2, features),
        mixer_input,
        decay_shift.T,
        input_map.swapaxes(2, 3).reshape(2, channels, states),
        readout.reshape(2, channels, states),
        mixer_weight,
        shared_gate,
        shared_up,
        shared_down,
        expert_switch_matrix.reshape(features, ff),
        up_weight.reshape(features, ff),
        down_weight.reshape(n_tp, 2, ff // 2, columns),
    )
    return tuple(pl.pallas_call(
        functools.partial(fused_kernel, n_ep, n_tp, states),
        out_shape=(
            jax.ShapeDtypeStruct((rows, mixer_weight.shape[1]), bf16),
            jax.ShapeDtypeStruct((count, columns), bf16),
        ),
        in_specs=[vmem] * 4 + [anywhere] * len(operands),
        out_specs=(vmem, vmem),
        scratch_shapes=[pltpu.VMEM(a.shape, a.dtype) for a in operands] + [
            pltpu.VMEM((4, merged), f32),
            pltpu.VMEM((rows, merged), f32),
            pltpu.VMEM((rows, merged), f32),
            pltpu.VMEM((rows, merged), f32),
            pltpu.VMEM((4, SUBLANES, merged), f32),
            pltpu.VMEM((n_ep, 4, merged), f32),
            pltpu.VMEM((n_tp, 2, rows // 2, channels), bf16),
            pltpu.VMEM((n_ep, 2, count // 2, features), bf16),
            pltpu.VMEM((n_ep, 2, count), jnp.int32),
            pltpu.VMEM((cap, features), bf16),
            pltpu.VMEM((n_ep, n_tp, 2, cap, ff // 2), bf16),
            pltpu.VMEM((n_ep, cap, columns), bf16),
            pltpu.VMEM((n_ep, cap, columns), bf16),
            pltpu.VMEM((n_tp, 2, count // 2, shared_ff), bf16),
            pltpu.VMEM((count, columns), f32),
            pltpu.VMEM((n_ep * cap, count), bf16),
            pltpu.VMEM((n_ep * cap, count), bf16),
            dma((len(operands),)), dma((n_ep, 2)), dma((n_ep, 2)), dma((2, 2)),
            dma((n_ep,)), dma((n_ep,)), dma((n_ep,)), dma((n_ep,)), dma((n_ep,)),
            dma((2, n_tp)), dma((n_tp, 2)), dma((n_ep, 2, n_tp)), dma((n_ep, n_tp, 2)),
            dma((n_ep,)), dma((n_ep,)), dma((2, n_tp)), dma((n_tp, 2)),
        ],
        compiler_params=pltpu.CompilerParams(
            collective_id=0, has_side_effects=True, vmem_limit_bytes=56 * 1024 * 1024
        ),
        name="fused",
    )(
        routes.T, route_weight.T, log_step.reshape(1, groups), norm_gain.reshape(1, features),
        *operands,
    ))


def solution(mesh):
    placed = (
        P("ep", "tp"),
        P("tp"),
        P("ep", "tp"),
        P(None, "tp", None, None),
        P(None, "tp", None, None),
        P(None, "tp"),
        P("ep", None),
        P(),
        P("ep", None),
        P("ep", None),
        P("ep", None, "tp"),
        P("ep", None, "tp"),
        P("ep", None, "tp"),
        P(None, "tp"),
        P(None, "tp"),
        P(None, "tp"),
    )
    return jax.shard_map(
        shards,
        mesh=mesh,
        in_specs=placed,
        out_specs=(P("ep", "tp"), P("ep", "tp")),
        check_vma=False,
    )
```

```python
import functools
import math

import jax
import jax.numpy as jnp
from jax import lax
from jax.experimental import pallas as pl
from jax.experimental.pallas import tpu as pltpu
from jax.sharding import PartitionSpec as P

MESH = pl.DeviceIdType.MESH
SUBLANES = 8
NT = (((1,), (1,)), ((), ()))
TN = (((0,), (0,)), ((), ()))


def times(ar, ai, br, bi):
    return ar * br - ai * bi, ar * bi + ai * br


def iota(shape, dim):
    return lax.broadcasted_iota(jnp.int32, shape, dim)


def spread(shape, period):
    return (iota(shape, 1) % period == iota(shape, 0)).astype(jnp.bfloat16)


def halves(a):
    high = a.astype(jnp.bfloat16)
    return high, (a - high.astype(jnp.float32)).astype(jnp.bfloat16)


def dot(a, b, dims=None):
    if dims is None:
        return jnp.dot(a, b, preferred_element_type=jnp.float32)
    return lax.dot_general(a, b, dims, preferred_element_type=jnp.float32)


def fill_table(rate_ref, table, states):
    groups = rate_ref.shape[1]
    merged = table.shape[1]
    same = iota((groups, groups), 0) == iota((groups, groups), 1)
    column = jnp.sum(jnp.where(same, rate_ref[...], 0.0), axis=1, keepdims=True)
    place = iota((groups, merged), 1) // states == iota((groups, merged), 0)
    wide = jnp.sum(jnp.where(place, column, 0.0), axis=0, keepdims=True)
    step_rate = jnp.exp(wide)
    frequency = jnp.pi * lax.rem(iota((1, merged), 1), states).astype(jnp.float32)
    angle = step_rate * frequency
    turn_cosine = jnp.cos(angle)
    turn_sine = jnp.sin(angle)
    base = jnp.exp(-0.5 * step_rate)
    starting_quadrature = base * turn_sine
    inverse = 1.0 / (0.25 + frequency * frequency)
    lowered = base * turn_cosine - 1.0
    table[0:1, :] = turn_cosine
    table[1:2, :] = turn_sine
    table[2:3, :] = (-0.5 * lowered + starting_quadrature * frequency) * inverse
    table[3:4, :] = (-0.5 * starting_quadrature - lowered * frequency) * inverse
    return column


def drive_into(x_ref, column, shift_ref, map_ref, table_ref, mag, push_re, push_im, states):
    rows, channels = x_ref.shape
    merged = mag.shape[1]
    groups = shift_ref.shape[0]
    width = channels // groups
    steps = rows // SUBLANES
    place = iota((rows, rows), 0)
    order = (iota((rows, rows), 1) == (place % SUBLANES) * steps + place // SUBLANES).astype(
        jnp.bfloat16
    )
    level = jnp.exp(-0.5 * jnp.exp(column) + shift_ref[...])
    high, middle = halves(level)
    low = ((level - high.astype(jnp.float32)) - middle.astype(jnp.float32)).astype(jnp.bfloat16)
    widen = (iota((groups, merged), 1) // states == iota((groups, merged), 0)).astype(jnp.bfloat16)
    total = None
    for piece in (high, middle, low):
        part = dot(dot(order, piece, NT).astype(jnp.bfloat16), widen)
        total = part if total is None else total + part
    mag[...] = total
    x = dot(order, x_ref[...]).astype(jnp.bfloat16)
    repeat = spread((states, merged), states)
    mine = iota((channels, merged), 1) // states == iota((channels, merged), 0) // width
    drives = []
    for c in range(2):
        wide = jnp.where(mine, dot(map_ref[c], repeat), 0.0).astype(jnp.bfloat16)
        drives.append(dot(x, wide))
    re, im = times(table_ref[2:3, :], table_ref[3:4, :], drives[0], drives[1])
    push_re[...] = re
    push_im[...] = im


def sweep(table_ref, mag, push_re, push_im, start_re, start_im, keep):
    rows, merged = mag.shape
    turn_re = jnp.broadcast_to(table_ref[0:1, :], (SUBLANES, merged))
    turn_im = jnp.broadcast_to(table_ref[1:2, :], (SUBLANES, merged))

    def one(j, carry):
        re, im, product = carry
        at = pl.ds(pl.multiple_of(j * SUBLANES, SUBLANES), SUBLANES)
        level = mag[at, :]
        next_re, next_im = times(turn_re, turn_im, re, im)
        next_re = level * next_re + push_re[at, :]
        next_im = level * next_im + push_im[at, :]
        if keep:
            push_re[at, :] = next_re
            push_im[at, :] = next_im
        else:
            product = product * level
        return next_re, next_im, product

    product = jnp.ones((SUBLANES, merged), jnp.float32)
    if keep:
        def pair(j, carry):
            return one(j, carry + (None,))[:2]
        return lax.fori_loop(0, rows // SUBLANES, pair, (start_re, start_im))
    return lax.fori_loop(0, rows // SUBLANES, one, (start_re, start_im, product))


def join(table_ref, ends_re, ends_im, product, pre, steps):
    merged = ends_re.shape[1]
    wr, wi = table_ref[0:1, :], table_ref[1:2, :]
    power = 1
    while power < steps:
        wr, wi = times(wr, wi, wr, wi)
        power *= 2
    cr = jnp.zeros((1, merged), jnp.float32)
    ci = cr
    ar = cr + 1.0
    ai = cr
    for s in range(SUBLANES):
        for i, v in enumerate((cr, ci, ar, ai)):
            pre[i, s : s + 1, :] = v
        level = product[s : s + 1]
        fr, fi = level * wr, level * wi
        tr, ti = times(fr, fi, cr, ci)
        cr, ci = tr + ends_re[s : s + 1], ti + ends_im[s : s + 1]
        ar, ai = times(fr, fi, ar, ai)
    return cr, ci, ar, ai


def read_states(readout_ref, push_re, push_im, states):
    rows, merged = push_re.shape
    channels = readout_ref.shape[1]
    width = channels * states // merged
    repeat = spread((states, merged), states)
    mine = iota((channels, merged), 1) // states == iota((channels, merged), 0) // width
    total = None
    for c, ref in enumerate((push_re, push_im)):
        high, low = halves(ref[...])
        back = readout_ref[c] if c == 0 else -readout_ref[c]
        wide_high, wide_low = (
            jnp.where(mine, dot(half, repeat), 0.0).astype(jnp.bfloat16) for half in halves(back)
        )
        part = dot(high, wide_high, NT) + (dot(low, wide_high, NT) + dot(high, wide_low, NT))
        total = part if total is None else total + part
    place = iota((rows, rows), 0)
    steps = rows // SUBLANES
    order = (iota((rows, rows), 1) == (place % steps) * SUBLANES + place // steps).astype(
        jnp.bfloat16
    )
    cube = total + 0.044715 * (total * total * total)
    active = (0.5 * total * (1.0 + jnp.tanh(0.7978845608028654 * cube))).astype(jnp.bfloat16)
    return dot(order, active).astype(jnp.bfloat16)


def remote(src, dst, send, recv, **target):
    return pltpu.make_async_remote_copy(
        src_ref=src, dst_ref=dst, send_sem=send, recv_sem=recv,
        device_id=target, device_id_type=MESH,
    )


def visits(chips):
    plan = []
    for chip in range(chips):
        end = chip in (0, chips - 1)
        found = []
        for d in range(1, chips):
            for j in range(2):
                for there, onward in ((chip - d, chip + 1), (chip + d, chip - 1)):
                    if 0 <= there < chips:
                        onward = onward if 0 <= onward < chips else -1
                        found.append((2 * there + j, onward, 2 * d + j))
        units = []
        for u, (source, onward, arrival) in enumerate(found):
            together = max(v for v in range(len(found)) if found[v][2] == arrival)
            step = 2 * u if end else max(0, 2 * together - 3)
            units.append((source, onward, step, int(end and u > 1)))
        plan.append(units)
    return plan


def fused_kernel(
    n_ep, n_tp, states,
    routes_ref, gains_ref, rate_ref, gain_ref,
    input_hbm, x_hbm, shift_hbm, map_hbm, readout_hbm, weight_hbm,
    sgate_hbm, sup_hbm, sdown_hbm, gate_hbm, up_hbm, down_hbm,
    out_ref, experts_ref,
    tokens, x_ref, shift_ref, map_ref, readout_ref, weight_ref,
    sgate, sup, sdown, gate, up, down,
    table, mag, push_re, push_im, pre, summary, active,
    tok, named, picked, hidden, result, returned, shared, common, high, low, out_v, experts_v,
    load, store, tok_recv, mate_send, own_send, on_send, n_send, n_recv,
    e_send, e_recv, a_send, a_recv, h_send, h_recv, r_send, r_recv, s_send, s_recv,
):
    ep = lax.axis_index("ep")
    tp = lax.axis_index("tp")
    rows, channels = x_ref.shape
    merged = mag.shape[1]
    half_rows, features = tok.shape[2:]
    count = 2 * half_rows
    cap = picked.shape[0] // 2
    chips = n_ep // 2
    chip, core = ep // 2, lax.rem(ep, 2)
    mate = ep + 1 - 2 * core
    side = math.isqrt(n_tp)
    y, x = tp // side, lax.rem(tp, side)
    half = hidden.shape[4]

    barrier = pltpu.get_barrier_semaphore()
    for d in range(1, n_ep):
        pl.semaphore_signal(
            barrier, inc=1, device_id={"ep": lax.rem(ep + d, n_ep)}, device_id_type=MESH
        )
    for d in range(1, n_tp):
        pl.semaphore_signal(
            barrier, inc=1, device_id={"tp": lax.rem(tp + d, n_tp)}, device_id_type=MESH
        )
    pairs = (
        (input_hbm, tokens), (sgate_hbm, sgate), (sup_hbm, sup), (gate_hbm, gate), (up_hbm, up),
        (x_hbm, x_ref), (shift_hbm, shift_ref), (map_hbm, map_ref), (down_hbm, down),
        (readout_hbm, readout_ref), (weight_hbm, weight_ref), (sdown_hbm, sdown),
    )
    loads = [pltpu.make_async_copy(a, b, load.at[i]) for i, (a, b) in enumerate(pairs)]
    for copy in loads:
        copy.start()
    store_out = pltpu.make_async_copy(out_v, out_ref, store.at[0])
    store_experts = pltpu.make_async_copy(experts_v, experts_ref, store.at[1])
    def across(dy, dx):
        return lax.rem(y + dy, side) * side + lax.rem(x + dx, side)

    peers = {(dy, dx): across(dy, dx) for dy in range(side) for dx in range(side)}

    class Share:
        def __init__(self, buffer, send, recv):
            self.buffer, self.send, self.recv = buffer, send, recv

        def copy(self, source, h, to, k):
            at = self.buffer.at[source, h]
            return remote(at, at, self.send, self.recv.at[k], tp=to)

        def start(self, h):
            for o in range(1, side):
                self.copy(tp, h, peers[0, o], 0 if h == 0 else 2).start()
                self.copy(tp, h, peers[o, 0], 1 if h == 1 else 2).start()

        def wait(self, at, k):
            remote(at, at, self.send, self.recv.at[k], tp=peers[0, 1]).wait_recv()

        def forward(self):
            for h in range(2):
                self.wait(self.buffer.at[pl.ds(0, side - 1), h], h)
                for o in range(1, side):
                    for d in range(1, side):
                        source, to = ((0, o), (d, 0)) if h == 0 else ((o, 0), (0, d))
                        self.copy(peers[source], h, peers[to], 3).start()

        def near(self):
            self.wait(self.buffer.at[pl.ds(0, side - 1)], 2)

        def far(self):
            self.wait(self.buffer.at[pl.ds(0, (side - 1) ** 2)], 3)

        def drain(self, at):
            remote(at, at, self.send, self.recv.at[0], tp=peers[0, 1]).wait_send()

    def hidden_of(s):
        return Share(hidden.at[s], h_send.at[0], h_recv.at[s])

    shared_out = Share(shared, s_send.at[0], s_recv)
    active_out = Share(active, a_send.at[0], a_recv)

    loads[0].wait()
    block = 16
    scale = gain_ref[...]

    @pl.loop(0, half_rows // block)
    def _(i):
        at = pl.ds(pl.multiple_of(i * block, block), block)
        for h in range(2):
            values = tokens[h, at, :].astype(jnp.float32)
            level = lax.rsqrt(jnp.mean(values * values, axis=-1, keepdims=True) + 1e-06)
            tok[ep, h, at, :] = (values * level * scale).astype(jnp.bfloat16)

    named[ep] = routes_ref[...]
    pl.semaphore_wait(barrier, n_ep + n_tp - 2)

    def piece(s, h, send, target):
        return remote(tok.at[s, h], tok.at[s, h], send, tok_recv.at[s, h], ep=target)

    piece(ep, 1 - core, mate_send.at[0], mate).start()
    piece(ep, core, mate_send.at[0], mate).start()
    remote(routes_ref, named.at[ep], n_send.at[0], n_recv.at[0], ep=mate).start()
    strangers = [
        2 * lax.rem(chip + d, chips) + c for d in range(1, chips) for c in range(2)
    ]
    for target in strangers:
        remote(routes_ref, named.at[ep], n_send.at[0], n_recv.at[1], ep=target).start()
    ends = ((chip > 0, lax.rem(ep + n_ep - 2, n_ep)), (chip < chips - 1, lax.rem(ep + 2, n_ep)))

    def own(j, d):
        return piece(2 * chip + j, core, own_send.at[d], ends[d][1])

    for j in range(2):
        @pl.when(core != j)
        def _():
            piece(2 * chip + j, core, mate_send.at[0], mate).wait_recv()

        for d in range(2):
            @pl.when(ends[d][0])
            def _():
                own(j, d).start()

    def shared_hidden():
        for copy in loads[1:3]:
            copy.wait()
        a = tok[ep].reshape(count, features)
        v = dot(a, sgate[...])
        shared[tp] = (v / (1.0 + jnp.exp(-v)) * dot(a, sup[...])).astype(jnp.bfloat16).reshape(
            shared.shape[1:]
        )
        for h in range(2):
            shared_out.start(h)

    later = (iota((count, count), 0) <= iota((count, count), 1)).astype(jnp.bfloat16)
    slots = iota((cap, count), 0).astype(jnp.float32)

    def member(names, expert):
        return jnp.logical_or(names[0:1] == expert, names[1:2] == expert)

    def seats(mine):
        ones = jnp.where(mine, 1.0, 0.0)
        ranks = dot(ones.astype(jnp.bfloat16), later)
        return jnp.where(mine, ranks - 1.0, -1.0)

    tile = min(half, 256)

    def process(*group):
        for i, s in enumerate(group):
            names = named[s]
            place = seats(jnp.broadcast_to(member(names, ep), (SUBLANES, count)))
            chosen = (slots == place[0:1]).astype(jnp.bfloat16)
            picked[i * cap : (i + 1) * cap, :] = dot(
                chosen, tok[s].reshape(count, features)
            ).astype(jnp.bfloat16)
        for h in range(2):
            @pl.loop(0, half // tile)
            def _(n):
                inner = pl.ds(pl.multiple_of(n * tile, tile), tile)
                at = pl.ds(pl.multiple_of(h * half + n * tile, tile), tile)
                a = picked[: len(group) * cap, :]
                v = dot(a, gate[:, at])
                v = (v / (1.0 + jnp.exp(-v)) * dot(a, up[:, at])).astype(jnp.bfloat16)
                for i, s in enumerate(group):
                    hidden[s, tp, h, :, inner] = v[i * cap : (i + 1) * cap]

            for s in group:
                hidden_of(s).start(h)

    def back(s):
        return remote(result.at[s], returned.at[ep], r_send.at[0], r_recv.at[0], ep=s)

    def project(*group, before=None):
        def part(q):
            total = None
            for h in range(2):
                a = jnp.concatenate([hidden[s, q, h] for s in group], axis=0)
                one = dot(a, down[q, h])
                total = one if total is None else total + one
            return total

        total = part(tp)
        if before is not None:
            before()
        for s in group:
            hidden_of(s).near()
        for o in range(1, side):
            total = total + part(peers[0, o])
            total = total + part(peers[o, 0])
        for s in group:
            hidden_of(s).far()
        for dy in range(1, side):
            for dx in range(1, side):
                total = total + part(peers[dy, dx])
        for i, s in enumerate(group):
            result[s] = total[i * cap : (i + 1) * cap].astype(jnp.bfloat16)
        if len(group) == 2:
            returned[ep] = result[ep]
            back(mate).start()
        else:
            back(group[0]).start()

    def scan_block():
        for copy in loads[5:8]:
            copy.wait()
        column = fill_table(rate_ref, table, states)
        drive_into(x_ref, column, shift_ref, map_ref, table, mag, push_re, push_im, states)
        zero = jnp.zeros((SUBLANES, merged), jnp.float32)
        ends_re, ends_im, product = sweep(table, mag, push_re, push_im, zero, zero, False)
        end = join(table, ends_re, ends_im, product, pre, rows // SUBLANES)
        for i, v in enumerate(end):
            summary[ep, i : i + 1, :] = v
        for target in strangers + [mate]:
            remote(
                summary.at[ep], summary.at[ep], e_send.at[0], e_recv.at[0], ep=target
            ).start()

    def gain_blocks():
        names = routes_ref[...]
        level = gains_ref[...]
        for e in range(n_ep):
            place = seats(jnp.broadcast_to(member(names, e), (SUBLANES, count)))
            weight = jnp.where(names[0:1] == e, level[0:1], 0.0) + jnp.where(
                names[1:2] == e, level[1:2], 0.0
            )
            wide = jnp.where(slots == place[0:1], weight, 0.0)
            top, rest = halves(wide)
            high[e * cap : (e + 1) * cap, :] = top
            low[e * cap : (e + 1) * cap, :] = rest

    def scan_states():
        rest = summary.at[pl.ds(0, n_ep - 1)]
        remote(rest, rest, e_send.at[0], e_recv.at[0], ep=mate).wait_recv()

        def fold(e, carry):
            part = summary[e]
            re, im = times(part[2:3], part[3:4], carry[0], carry[1])
            return re + part[0:1], im + part[1:2]

        nothing = jnp.zeros((1, merged), jnp.float32)
        in_re, in_im = lax.fori_loop(0, ep, fold, (nothing, nothing))
        add_re, add_im = times(pre[2], pre[3], in_re, in_im)
        sweep(table, mag, push_re, push_im, pre[0] + add_re, pre[1] + add_im, True)
        loads[9].wait()
        active[tp] = read_states(readout_ref, push_re, push_im, states).reshape(active.shape[1:])
        for h in range(2):
            active_out.start(h)

    def mix():
        active_out.near()
        active_out.far()
        loads[10].wait()
        total = None
        for q in range(n_tp):
            a = active[q].reshape(rows, channels)
            part = dot(a, weight_ref[q * channels : (q + 1) * channels, :])
            total = part if total is None else total + part
        out_v[...] = total.astype(out_v.dtype)
        store_out.start()
        shared_out.near()
        shared_out.far()
        loads[11].wait()
        width = shared.shape[3]
        total = None
        for q in range(n_tp):
            a = shared[q].reshape(count, width)
            part = dot(a, sdown[q * width : (q + 1) * width, :])
            total = part if total is None else total + part
        common[...] = total

    plan = visits(chips)
    last = len(plan[0]) - 1

    def here(u, field):
        value = jnp.int32(plan[0][u][field])
        for k in range(1, chips):
            value = jnp.where(chip == k, jnp.int32(plan[k][u][field]), value)
        return value

    source = [here(u, 0) for u in range(last + 1)]
    onward = [here(u, 1) for u in range(last + 1)]
    steps = [here(u, 2) for u in range(last + 1)]
    early = [here(u, 3) for u in range(last + 1)]

    def along(u):
        target = 2 * jnp.maximum(onward[u], 0) + core
        return piece(source[u], core, on_send.at[0], target)

    def aside(u):
        return piece(source[u], core, mate_send.at[0], mate)

    def pass_on(u):
        aside(u).wait_recv()

        @pl.when(onward[u] >= 0)
        def _():
            along(u).start()

        aside(u).start()

    def ready(s):
        piece(s, 1 - core, mate_send.at[0], mate).wait_recv()

    groups = [(2 * chip, 2 * chip + 1)] + [(s,) for s in source]

    def forward(group):
        for s in group:
            hidden_of(s).forward()

    shared_hidden()
    for copy in loads[3:5]:
        copy.wait()
    ready(mate)
    remote(routes_ref, named.at[mate], n_send.at[0], n_recv.at[0], ep=mate).wait_recv()
    process(*groups[0])
    scan_block()
    gain_blocks()
    shared_out.forward()
    rest = named.at[pl.ds(0, n_ep - 2)]
    remote(rest, rest, n_send.at[0], n_recv.at[1], ep=mate).wait_recv()

    def arrivals(step):
        for v in range(last + 1):
            if any(units[v][2] == step for units in plan):
                @pl.when(steps[v] == step)
                def _():
                    pass_on(v)

    for u in range(last + 1):
        arrivals(2 * u)

        @pl.when(early[u] == 1)
        def _():
            forward(groups[u])

        ready(source[u])
        process(source[u])
        arrivals(2 * u + 1)

        @pl.when(early[u] == 0)
        def _():
            forward(groups[u])

        if u == 1:
            loads[8].wait()
        if u > 0:
            project(*groups[u - 1])
        if u == min(2, last):
            scan_states()
        if u == min(3, last):
            active_out.forward()
        if u == min(4, last):
            mix()
    project(*groups[last])
    project(*groups[last + 1], before=functools.partial(forward, groups[last + 1]))
    rest = returned.at[pl.ds(0, n_ep - 1)]
    remote(rest, rest, r_send.at[0], r_recv.at[0], ep=mate).wait_recv()
    back_rows = returned[...].reshape(n_ep * cap, returned.shape[2])
    routed = dot(high[...], back_rows, TN) + dot(low[...], back_rows, TN)
    experts_v[...] = (common[...] + routed).astype(experts_v.dtype)
    store_experts.start()
    shared_out.drain(shared.at[pl.ds(0, n_tp - 1)])
    active_out.drain(active.at[pl.ds(0, n_tp - 1)])
    hidden_of(ep).drain(hidden.at[:, pl.ds(0, n_tp - 1)])

    def drain(at, send, recv):
        remote(at, at, send, recv, ep=mate).wait_send()

    drain(named.at[pl.ds(0, n_ep - 1)], n_send.at[0], n_recv.at[0])
    drain(summary.at[pl.ds(0, n_ep - 1)], e_send.at[0], e_recv.at[0])
    drain(result.at[pl.ds(0, n_ep - 1)], r_send.at[0], r_recv.at[0])
    drain(tok.at[:, 0], mate_send.at[0], tok_recv.at[0, 0])
    for d in range(2):
        @pl.when(ends[d][0])
        def _():
            drain(tok.at[pl.ds(0, 2), 0], own_send.at[d], tok_recv.at[0, 0])

    @pl.when(jnp.logical_and(ends[0][0], ends[1][0]))
    def _():
        drain(tok.at[pl.ds(0, last + 1), 0], on_send.at[0], tok_recv.at[0, 0])

    store_out.wait()
    store_experts.wait()


def shards(
    mixer_input,
    log_step,
    decay_shift,
    input_map,
    readout,
    mixer_weight,
    expert_input,
    norm_gain,
    routes,
    route_weight,
    expert_switch_matrix,
    up_weight,
    down_weight,
    shared_gate,
    shared_up,
    shared_down,
):
    n_ep, n_tp = lax.axis_size("ep"), lax.axis_size("tp")
    count, features = expert_input.shape
    cap = 2 * count * routes.shape[1] // n_ep
    rows, channels = mixer_input.shape
    groups = log_step.shape[0]
    states, width = input_map.shape[2:]
    merged = groups * states
    f32, bf16 = jnp.float32, jnp.bfloat16
    ff = up_weight.shape[2]
    depth, columns = down_weight.shape[1:]
    shared_ff = shared_up.shape[1]
    vmem = pl.BlockSpec(memory_space=pltpu.VMEM)
    anywhere = pl.BlockSpec(memory_space=pl.ANY)
    dma = pltpu.SemaphoreType.DMA
    operands = (
        expert_input.reshape(2, count // 2, features),
        mixer_input,
        decay_shift.T,
        input_map.swapaxes(2, 3).reshape(2, channels, states),
        readout.reshape(2, channels, states),
        mixer_weight,
        shared_gate,
        shared_up,
        shared_down,
        expert_switch_matrix.reshape(features, ff),
        up_weight.reshape(features, ff),
        down_weight.reshape(n_tp, 2, ff // 2, columns),
    )
    return tuple(pl.pallas_call(
        functools.partial(fused_kernel, n_ep, n_tp, states),
        out_shape=(
            jax.ShapeDtypeStruct((rows, mixer_weight.shape[1]), bf16),
            jax.ShapeDtypeStruct((count, columns), bf16),
        ),
        in_specs=[vmem] * 4 + [anywhere] * len(operands),
        out_specs=(anywhere, anywhere),
        scratch_shapes=[pltpu.VMEM(a.shape, a.dtype) for a in operands] + [
            pltpu.VMEM((4, merged), f32),
            pltpu.VMEM((rows, merged), f32),
            pltpu.VMEM((rows, merged), f32),
            pltpu.VMEM((rows, merged), f32),
            pltpu.VMEM((4, SUBLANES, merged), f32),
            pltpu.VMEM((n_ep, 4, merged), f32),
            pltpu.VMEM((n_tp, 2, rows // 2, channels), bf16),
            pltpu.VMEM((n_ep, 2, count // 2, features), bf16),
            pltpu.VMEM((n_ep, 2, count), jnp.int32),
            pltpu.VMEM((2 * cap, features), bf16),
            pltpu.VMEM((n_ep, n_tp, 2, cap, ff // 2), bf16),
            pltpu.VMEM((n_ep, cap, columns), bf16),
            pltpu.VMEM((n_ep, cap, columns), bf16),
            pltpu.VMEM((n_tp, 2, count // 2, shared_ff), bf16),
            pltpu.VMEM((count, columns), f32),
            pltpu.VMEM((n_ep * cap, count), bf16),
            pltpu.VMEM((n_ep * cap, count), bf16),
            pltpu.VMEM((rows, mixer_weight.shape[1]), bf16),
            pltpu.VMEM((count, columns), bf16),
            dma((len(operands),)), dma((2,)), dma((n_ep, 2)), dma((1,)), dma((2,)), dma((1,)),
            dma((1,)), dma((2,)), dma((1,)), dma((1,)), dma((1,)), dma((4,)),
            dma((1,)), dma((n_ep, 4)), dma((1,)), dma((1,)), dma((1,)), dma((4,)),
        ],
        compiler_params=pltpu.CompilerParams(
            collective_id=0, has_side_effects=True, vmem_limit_bytes=56 * 1024 * 1024
        ),
        name="fused",
    )(
        routes.T, route_weight.T, log_step.reshape(1, groups), norm_gain.reshape(1, features),
        *operands,
    ))


def solution(mesh):
    placed = (
        P("ep", "tp"),
        P("tp"),
        P("ep", "tp"),
        P(None, "tp", None, None),
        P(None, "tp", None, None),
        P(None, "tp"),
        P("ep", None),
        P(),
        P("ep", None),
        P("ep", None),
        P("ep", None, "tp"),
        P("ep", None, "tp"),
        P("ep", None, "tp"),
        P(None, "tp"),
        P(None, "tp"),
        P(None, "tp"),
    )
    return jax.shard_map(
        shards,
        mesh=mesh,
        in_specs=placed,
        out_specs=(P("ep", "tp"), P("ep", "tp")),
        check_vma=False,
    )
```

```python
import functools
import math

import jax
import jax.numpy as jnp
from jax import lax
from jax.experimental import pallas as pl
from jax.experimental.pallas import tpu as pltpu
from jax.sharding import PartitionSpec as P

MESH = pl.DeviceIdType.MESH
SUBLANES = 8
NT = (((1,), (1,)), ((), ()))
TN = (((0,), (0,)), ((), ()))


def times(ar, ai, br, bi):
    return ar * br - ai * bi, ar * bi + ai * br


def iota(shape, dim):
    return lax.broadcasted_iota(jnp.int32, shape, dim)


def spread(shape, period):
    return (iota(shape, 1) % period == iota(shape, 0)).astype(jnp.bfloat16)


def halves(a):
    high = a.astype(jnp.bfloat16)
    return high, (a - high.astype(jnp.float32)).astype(jnp.bfloat16)


def dot(a, b, dims=None):
    if dims is None:
        return jnp.dot(a, b, preferred_element_type=jnp.float32)
    return lax.dot_general(a, b, dims, preferred_element_type=jnp.float32)


def fill_table(rate_ref, table, states):
    groups = rate_ref.shape[1]
    merged = table.shape[1]
    same = iota((groups, groups), 0) == iota((groups, groups), 1)
    column = jnp.sum(jnp.where(same, rate_ref[...], 0.0), axis=1, keepdims=True)
    place = iota((groups, merged), 1) // states == iota((groups, merged), 0)
    wide = jnp.sum(jnp.where(place, column, 0.0), axis=0, keepdims=True)
    step_rate = jnp.exp(wide)
    frequency = jnp.pi * lax.rem(iota((1, merged), 1), states).astype(jnp.float32)
    angle = step_rate * frequency
    turn_cosine = jnp.cos(angle)
    turn_sine = jnp.sin(angle)
    base = jnp.exp(-0.5 * step_rate)
    starting_quadrature = base * turn_sine
    inverse = 1.0 / (0.25 + frequency * frequency)
    lowered = base * turn_cosine - 1.0
    table[0:1, :] = turn_cosine
    table[1:2, :] = turn_sine
    table[2:3, :] = (-0.5 * lowered + starting_quadrature * frequency) * inverse
    table[3:4, :] = (-0.5 * starting_quadrature - lowered * frequency) * inverse
    return column


def drive_into(x_ref, column, shift_ref, map_ref, table_ref, mag, push_re, push_im, states):
    rows, channels = x_ref.shape
    merged = mag.shape[1]
    groups = shift_ref.shape[0]
    width = channels // groups
    steps = rows // SUBLANES
    place = iota((rows, rows), 0)
    order = (iota((rows, rows), 1) == (place % SUBLANES) * steps + place // SUBLANES).astype(
        jnp.bfloat16
    )
    level = jnp.exp(-0.5 * jnp.exp(column) + shift_ref[...])
    high, middle = halves(level)
    low = ((level - high.astype(jnp.float32)) - middle.astype(jnp.float32)).astype(jnp.bfloat16)
    widen = (iota((groups, merged), 1) // states == iota((groups, merged), 0)).astype(jnp.bfloat16)
    total = None
    for piece in (high, middle, low):
        part = dot(dot(order, piece, NT).astype(jnp.bfloat16), widen)
        total = part if total is None else total + part
    mag[...] = total
    x = dot(order, x_ref[...]).astype(jnp.bfloat16)
    repeat = spread((states, merged), states)
    mine = iota((channels, merged), 1) // states == iota((channels, merged), 0) // width
    drives = []
    for c in range(2):
        wide = jnp.where(mine, dot(map_ref[c], repeat), 0.0).astype(jnp.bfloat16)
        drives.append(dot(x, wide))
    re, im = times(table_ref[2:3, :], table_ref[3:4, :], drives[0], drives[1])
    push_re[...] = re
    push_im[...] = im


def sweep(table_ref, mag, push_re, push_im, start_re, start_im, keep):
    rows, merged = mag.shape
    turn_re = jnp.broadcast_to(table_ref[0:1, :], (SUBLANES, merged))
    turn_im = jnp.broadcast_to(table_ref[1:2, :], (SUBLANES, merged))

    def one(j, carry):
        re, im, product = carry
        at = pl.ds(pl.multiple_of(j * SUBLANES, SUBLANES), SUBLANES)
        level = mag[at, :]
        next_re, next_im = times(turn_re, turn_im, re, im)
        next_re = level * next_re + push_re[at, :]
        next_im = level * next_im + push_im[at, :]
        if keep:
            push_re[at, :] = next_re
            push_im[at, :] = next_im
        else:
            product = product * level
        return next_re, next_im, product

    product = jnp.ones((SUBLANES, merged), jnp.float32)
    if keep:
        def pair(j, carry):
            return one(j, carry + (None,))[:2]
        return lax.fori_loop(0, rows // SUBLANES, pair, (start_re, start_im))
    return lax.fori_loop(0, rows // SUBLANES, one, (start_re, start_im, product))


def join(table_ref, ends_re, ends_im, product, pre, steps):
    merged = ends_re.shape[1]
    wr, wi = table_ref[0:1, :], table_ref[1:2, :]
    power = 1
    while power < steps:
        wr, wi = times(wr, wi, wr, wi)
        power *= 2
    cr = jnp.zeros((1, merged), jnp.float32)
    ci = cr
    ar = cr + 1.0
    ai = cr
    for s in range(SUBLANES):
        for i, v in enumerate((cr, ci, ar, ai)):
            pre[i, s : s + 1, :] = v
        level = product[s : s + 1]
        fr, fi = level * wr, level * wi
        tr, ti = times(fr, fi, cr, ci)
        cr, ci = tr + ends_re[s : s + 1], ti + ends_im[s : s + 1]
        ar, ai = times(fr, fi, ar, ai)
    return cr, ci, ar, ai


def read_states(readout_ref, push_re, push_im, states):
    rows, merged = push_re.shape
    channels = readout_ref.shape[1]
    width = channels * states // merged
    repeat = spread((states, merged), states)
    mine = iota((channels, merged), 1) // states == iota((channels, merged), 0) // width
    total = None
    for c, ref in enumerate((push_re, push_im)):
        high, low = halves(ref[...])
        back = readout_ref[c] if c == 0 else -readout_ref[c]
        wide_high, wide_low = (
            jnp.where(mine, dot(half, repeat), 0.0).astype(jnp.bfloat16) for half in halves(back)
        )
        part = dot(high, wide_high, NT) + (dot(low, wide_high, NT) + dot(high, wide_low, NT))
        total = part if total is None else total + part
    place = iota((rows, rows), 0)
    steps = rows // SUBLANES
    order = (iota((rows, rows), 1) == (place % steps) * SUBLANES + place // steps).astype(
        jnp.bfloat16
    )
    cube = total + 0.044715 * (total * total * total)
    active = (0.5 * total * (1.0 + jnp.tanh(0.7978845608028654 * cube))).astype(jnp.bfloat16)
    return dot(order, active).astype(jnp.bfloat16)


def remote(src, dst, send, recv, **target):
    return pltpu.make_async_remote_copy(
        src_ref=src, dst_ref=dst, send_sem=send, recv_sem=recv,
        device_id=target, device_id_type=MESH,
    )


def visits(chips):
    plan = []
    for chip in range(chips):
        end = chip in (0, chips - 1)
        found = []
        for d in range(1, chips):
            for j in range(2):
                for there, onward in ((chip - d, chip + 1), (chip + d, chip - 1)):
                    if 0 <= there < chips:
                        onward = onward if 0 <= onward < chips else -1
                        found.append((2 * there + j, onward, 2 * d + j))
        units = []
        for u, (source, onward, arrival) in enumerate(found):
            together = max(v for v in range(len(found)) if found[v][2] == arrival)
            ahead = max((3 * together - 1) // 2, 3 * together - 7) if together > 1 else 0
            units.append((source, onward, 3 * u if end else ahead))
        plan.append(units)
    return plan


def fused_kernel(
    n_ep, n_tp, states,
    routes_ref, gains_ref, rate_ref, gain_ref,
    input_hbm, x_hbm, shift_hbm, map_hbm, readout_hbm, weight_hbm,
    sgate_hbm, sup_hbm, sdown_hbm, gate_hbm, up_hbm, down_hbm,
    out_ref, experts_ref,
    tokens, x_ref, shift_ref, map_ref, readout_ref, weight_ref,
    sgate, sup, sdown, gate, up, down,
    table, mag, push_re, push_im, pre, summary, active,
    tok, named, ranks, picked, hidden, result, returned, shared, common, high, low,
    load, tok_recv, mate_send, own_send, on_send, n_send, n_recv,
    e_send, e_recv, a_send, a_recv, h_send, h_recv, r_send, r_recv, s_send, s_recv,
):
    ep = lax.axis_index("ep")
    tp = lax.axis_index("tp")
    rows, channels = x_ref.shape
    merged = mag.shape[1]
    half_rows, features = tok.shape[2:]
    count = 2 * half_rows
    cap = picked.shape[0] // 2
    chips = n_ep // 2
    chip, core = ep // 2, lax.rem(ep, 2)
    mate = ep + 1 - 2 * core
    side = math.isqrt(n_tp)
    y, x = tp // side, lax.rem(tp, side)
    half = hidden.shape[4]

    barrier = pltpu.get_barrier_semaphore()
    for d in range(1, n_ep):
        pl.semaphore_signal(
            barrier, inc=1, device_id={"ep": lax.rem(ep + d, n_ep)}, device_id_type=MESH
        )
    for d in range(1, n_tp):
        pl.semaphore_signal(
            barrier, inc=1, device_id={"tp": lax.rem(tp + d, n_tp)}, device_id_type=MESH
        )
    pairs = (
        (input_hbm, tokens), (sgate_hbm, sgate), (sup_hbm, sup), (gate_hbm, gate), (up_hbm, up),
        (x_hbm, x_ref), (shift_hbm, shift_ref), (map_hbm, map_ref), (down_hbm, down),
        (readout_hbm, readout_ref), (weight_hbm, weight_ref), (sdown_hbm, sdown),
    )
    loads = [pltpu.make_async_copy(a, b, load.at[i]) for i, (a, b) in enumerate(pairs)]
    for copy in loads:
        copy.start()
    def across(dy, dx):
        return lax.rem(y + dy, side) * side + lax.rem(x + dx, side)

    peers = {(dy, dx): across(dy, dx) for dy in range(side) for dx in range(side)}

    class Share:
        def __init__(self, buffer, send, recv):
            self.buffer, self.send, self.recv = buffer, send, recv

        def copy(self, source, h, to, k):
            at = self.buffer.at[source, h]
            return remote(at, at, self.send, self.recv.at[k], tp=to)

        def start(self, h):
            for o in range(1, side):
                self.copy(tp, h, peers[0, o], 0 if h == 0 else 2).start()
                self.copy(tp, h, peers[o, 0], 1 if h == 1 else 2).start()

        def wait(self, at, k):
            remote(at, at, self.send, self.recv.at[k], tp=peers[0, 1]).wait_recv()

        def forward(self):
            for h in range(2):
                self.wait(self.buffer.at[pl.ds(0, side - 1), h], h)
                for o in range(1, side):
                    for d in range(1, side):
                        source, to = ((0, o), (d, 0)) if h == 0 else ((o, 0), (0, d))
                        self.copy(peers[source], h, peers[to], 3).start()

        def near(self):
            self.wait(self.buffer.at[pl.ds(0, side - 1)], 2)

        def far(self):
            self.wait(self.buffer.at[pl.ds(0, (side - 1) ** 2)], 3)

        def drain(self, at):
            remote(at, at, self.send, self.recv.at[0], tp=peers[0, 1]).wait_send()

    def hidden_of(s):
        return Share(hidden.at[s], h_send.at[0], h_recv.at[s])

    shared_out = Share(shared, s_send.at[0], s_recv)
    active_out = Share(active, a_send.at[0], a_recv)

    loads[0].wait()
    block = 16
    scale = gain_ref[...]

    @pl.loop(0, half_rows // block)
    def _(i):
        at = pl.ds(pl.multiple_of(i * block, block), block)
        for h in range(2):
            values = tokens[h, at, :].astype(jnp.float32)
            level = lax.rsqrt(jnp.mean(values * values, axis=-1, keepdims=True) + 1e-06)
            tok[ep, h, at, :] = (values * level * scale).astype(jnp.bfloat16)

    named[ep] = routes_ref[...]
    pl.semaphore_wait(barrier, n_ep + n_tp - 2)

    def piece(s, h, send, target):
        return remote(tok.at[s, h], tok.at[s, h], send, tok_recv.at[s, h], ep=target)

    piece(ep, 1 - core, mate_send.at[0], mate).start()
    piece(ep, core, mate_send.at[0], mate).start()
    remote(routes_ref, named.at[ep], n_send.at[0], n_recv.at[0], ep=mate).start()
    strangers = [
        2 * lax.rem(chip + d, chips) + c for d in range(1, chips) for c in range(2)
    ]
    for target in strangers:
        remote(routes_ref, named.at[ep], n_send.at[0], n_recv.at[1], ep=target).start()
    ends = ((chip > 0, lax.rem(ep + n_ep - 2, n_ep)), (chip < chips - 1, lax.rem(ep + 2, n_ep)))

    def own(j, d):
        return piece(2 * chip + j, core, own_send.at[d], ends[d][1])

    def depart(j):
        @pl.when(core != j)
        def _():
            piece(2 * chip + j, core, mate_send.at[0], mate).wait_recv()

        for d in range(2):
            @pl.when(ends[d][0])
            def _():
                own(j, d).start()

    depart(0)

    def shared_hidden():
        for copy in loads[1:3]:
            copy.wait()
        a = tok[ep].reshape(count, features)
        v = dot(a, sgate[...])
        shared[tp] = (v / (1.0 + jnp.exp(-v)) * dot(a, sup[...])).astype(jnp.bfloat16).reshape(
            shared.shape[1:]
        )
        for h in range(2):
            shared_out.start(h)

    later = (iota((count, count), 0) <= iota((count, count), 1)).astype(jnp.bfloat16)
    slots = iota((cap, count), 0).astype(jnp.float32)

    def member(names, expert):
        return jnp.where(jnp.logical_or(names[0:1] == expert, names[1:2] == expert), 1.0, 0.0)

    def seats(mine):
        return jnp.where(mine > 0.0, dot(mine.astype(jnp.bfloat16), later) - 1.0, -1.0)

    tile = half

    def process(*group):
        for i, s in enumerate(group):
            chosen = (slots == ranks[s]).astype(jnp.bfloat16)
            picked[i * cap : (i + 1) * cap, :] = dot(
                chosen, tok[s].reshape(count, features)
            ).astype(jnp.bfloat16)
        for h in range(2):
            @pl.loop(0, half // tile)
            def _(n):
                inner = pl.ds(pl.multiple_of(n * tile, tile), tile)
                at = pl.ds(pl.multiple_of(h * half + n * tile, tile), tile)
                a = picked[: len(group) * cap, :]
                v = dot(a, gate[:, at])
                v = (v / (1.0 + jnp.exp(-v)) * dot(a, up[:, at])).astype(jnp.bfloat16)
                for i, s in enumerate(group):
                    hidden[s, tp, h, :, inner] = v[i * cap : (i + 1) * cap]

            for s in group:
                hidden_of(s).start(h)

    def back(s):
        return remote(result.at[s], returned.at[ep], r_send.at[0], r_recv.at[0], ep=s)

    def project(*group):
        def part(q):
            total = None
            for h in range(2):
                a = jnp.concatenate([hidden[s, q, h] for s in group], axis=0)
                one = dot(a, down[q, h])
                total = one if total is None else total + one
            return total

        total = part(tp)
        for s in group:
            hidden_of(s).near()
        for o in range(1, side):
            total = total + part(peers[0, o])
            total = total + part(peers[o, 0])
        for s in group:
            hidden_of(s).far()
        for dy in range(1, side):
            for dx in range(1, side):
                total = total + part(peers[dy, dx])
        for i, s in enumerate(group):
            result[s] = total[i * cap : (i + 1) * cap].astype(jnp.bfloat16)
        if len(group) == 2:
            returned[ep] = result[ep]
            back(mate).start()
        else:
            back(group[0]).start()

    def scan_block():
        for copy in loads[5:8]:
            copy.wait()
        column = fill_table(rate_ref, table, states)
        drive_into(x_ref, column, shift_ref, map_ref, table, mag, push_re, push_im, states)
        zero = jnp.zeros((SUBLANES, merged), jnp.float32)
        ends_re, ends_im, product = sweep(table, mag, push_re, push_im, zero, zero, False)
        end = join(table, ends_re, ends_im, product, pre, rows // SUBLANES)
        for i, v in enumerate(end):
            summary[ep, i : i + 1, :] = v
        for target in strangers + [mate]:
            remote(
                summary.at[ep], summary.at[ep], e_send.at[0], e_recv.at[0], ep=target
            ).start()

    def rank(first, number):
        mine = [member(named[first + i], ep) for i in range(number)]
        mine += [mine[0]] * (-number % SUBLANES)
        place = seats(jnp.concatenate(mine, axis=0))
        for i in range(number):
            ranks[first + i] = place[i : i + 1]

    def gain_blocks():
        names = routes_ref[...]
        level = gains_ref[...]
        wanted = [member(names, e) for e in range(n_ep)]
        wanted += [wanted[0]] * (-n_ep % SUBLANES)
        places = seats(jnp.concatenate(wanted, axis=0))
        for e in range(n_ep):
            weight = jnp.where(names[0:1] == e, level[0:1], 0.0) + jnp.where(
                names[1:2] == e, level[1:2], 0.0
            )
            wide = jnp.where(slots == places[e : e + 1], weight, 0.0)
            top, rest = halves(wide)
            high[e * cap : (e + 1) * cap, :] = top
            low[e * cap : (e + 1) * cap, :] = rest

    def scan_states():
        rest = summary.at[pl.ds(0, n_ep - 1)]
        remote(rest, rest, e_send.at[0], e_recv.at[0], ep=mate).wait_recv()

        def fold(e, carry):
            part = summary[e]
            re, im = times(part[2:3], part[3:4], carry[0], carry[1])
            return re + part[0:1], im + part[1:2]

        nothing = jnp.zeros((1, merged), jnp.float32)
        in_re, in_im = lax.fori_loop(0, ep, fold, (nothing, nothing))
        add_re, add_im = times(pre[2], pre[3], in_re, in_im)
        sweep(table, mag, push_re, push_im, pre[0] + add_re, pre[1] + add_im, True)
        loads[9].wait()
        active[tp] = read_states(readout_ref, push_re, push_im, states).reshape(active.shape[1:])
        for h in range(2):
            active_out.start(h)

    def mix():
        active_out.near()
        active_out.far()
        loads[10].wait()
        total = None
        for q in range(n_tp):
            a = active[q].reshape(rows, channels)
            part = dot(a, weight_ref[q * channels : (q + 1) * channels, :])
            total = part if total is None else total + part
        out_ref[...] = total.astype(out_ref.dtype)
        shared_out.near()
        shared_out.far()
        loads[11].wait()
        width = shared.shape[3]
        total = None
        for q in range(n_tp):
            a = shared[q].reshape(count, width)
            part = dot(a, sdown[q * width : (q + 1) * width, :])
            total = part if total is None else total + part
        common[...] = total

    plan = visits(chips)
    last = len(plan[0]) - 1

    def here(u, field):
        value = jnp.int32(plan[0][u][field])
        for k in range(1, chips):
            value = jnp.where(chip == k, jnp.int32(plan[k][u][field]), value)
        return value

    source = [here(u, 0) for u in range(last + 1)]
    onward = [here(u, 1) for u in range(last + 1)]
    steps = [here(u, 2) for u in range(last + 1)]

    def along(u):
        target = 2 * jnp.maximum(onward[u], 0) + core
        return piece(source[u], core, on_send.at[0], target)

    def aside(u):
        return piece(source[u], core, mate_send.at[0], mate)

    def pass_on(u):
        aside(u).wait_recv()

        @pl.when(onward[u] >= 0)
        def _():
            along(u).start()

        aside(u).start()

    def ready(s):
        piece(s, 1 - core, mate_send.at[0], mate).wait_recv()

    groups = [(2 * chip, 2 * chip + 1)] + [(s,) for s in source]

    def forward(group):
        for s in group:
            hidden_of(s).forward()

    shared_hidden()
    depart(1)
    for copy in loads[3:5]:
        copy.wait()
    ready(mate)
    remote(routes_ref, named.at[mate], n_send.at[0], n_recv.at[0], ep=mate).wait_recv()
    rank(2 * chip, 2)
    process(*groups[0])
    scan_block()
    gain_blocks()
    shared_out.forward()
    rest = named.at[pl.ds(0, n_ep - 2)]
    remote(rest, rest, n_send.at[0], n_recv.at[1], ep=mate).wait_recv()
    rank(0, n_ep)

    def arrivals(step):
        for v in range(last + 1):
            if any(units[v][2] == step for units in plan):
                @pl.when(steps[v] == step)
                def _():
                    pass_on(v)

    for u in range(last + 1):
        arrivals(3 * u)
        if u == last:
            forward(groups[u])
        ready(source[u])
        process(source[u])
        arrivals(3 * u + 1)
        if u == min(1, last):
            scan_states()
        if u < last:
            forward(groups[u])
        if u == min(2, last):
            active_out.forward()
        if u == 1:
            loads[8].wait()
        if u > 0:
            project(*groups[u - 1])
        arrivals(3 * u + 2)
        if u == min(4, last):
            mix()
    forward(groups[last + 1])
    project(*groups[last])
    project(*groups[last + 1])
    rest = returned.at[pl.ds(0, n_ep - 1)]
    remote(rest, rest, r_send.at[0], r_recv.at[0], ep=mate).wait_recv()
    back_rows = returned[...].reshape(n_ep * cap, returned.shape[2])
    routed = dot(high[...], back_rows, TN) + dot(low[...], back_rows, TN)
    experts_ref[...] = (common[...] + routed).astype(experts_ref.dtype)
    shared_out.drain(shared.at[pl.ds(0, n_tp - 1)])
    active_out.drain(active.at[pl.ds(0, n_tp - 1)])
    hidden_of(ep).drain(hidden.at[:, pl.ds(0, n_tp - 1)])

    def drain(at, send, recv):
        remote(at, at, send, recv, ep=mate).wait_send()

    drain(named.at[pl.ds(0, n_ep - 1)], n_send.at[0], n_recv.at[0])
    drain(summary.at[pl.ds(0, n_ep - 1)], e_send.at[0], e_recv.at[0])
    drain(result.at[pl.ds(0, n_ep - 1)], r_send.at[0], r_recv.at[0])
    drain(tok.at[:, 0], mate_send.at[0], tok_recv.at[0, 0])
    for d in range(2):
        @pl.when(ends[d][0])
        def _():
            drain(tok.at[pl.ds(0, 2), 0], own_send.at[d], tok_recv.at[0, 0])

    @pl.when(jnp.logical_and(ends[0][0], ends[1][0]))
    def _():
        drain(tok.at[pl.ds(0, last + 1), 0], on_send.at[0], tok_recv.at[0, 0])


def shards(
    mixer_input,
    log_step,
    decay_shift,
    input_map,
    readout,
    mixer_weight,
    expert_input,
    norm_gain,
    routes,
    route_weight,
    expert_switch_matrix,
    up_weight,
    down_weight,
    shared_gate,
    shared_up,
    shared_down,
):
    n_ep, n_tp = lax.axis_size("ep"), lax.axis_size("tp")
    count, features = expert_input.shape
    cap = 2 * count * routes.shape[1] // n_ep
    rows, channels = mixer_input.shape
    groups = log_step.shape[0]
    states, width = input_map.shape[2:]
    merged = groups * states
    f32, bf16 = jnp.float32, jnp.bfloat16
    ff = up_weight.shape[2]
    depth, columns = down_weight.shape[1:]
    shared_ff = shared_up.shape[1]
    vmem = pl.BlockSpec(memory_space=pltpu.VMEM)
    anywhere = pl.BlockSpec(memory_space=pl.ANY)
    dma = pltpu.SemaphoreType.DMA
    operands = (
        expert_input.reshape(2, count // 2, features),
        mixer_input,
        decay_shift.T,
        input_map.swapaxes(2, 3).reshape(2, channels, states),
        readout.reshape(2, channels, states),
        mixer_weight,
        shared_gate,
        shared_up,
        shared_down,
        expert_switch_matrix.reshape(features, ff),
        up_weight.reshape(features, ff),
        down_weight.reshape(n_tp, 2, ff // 2, columns),
    )
    return tuple(pl.pallas_call(
        functools.partial(fused_kernel, n_ep, n_tp, states),
        out_shape=(
            pltpu.VMEM((rows, mixer_weight.shape[1]), bf16),
            pltpu.VMEM((count, columns), bf16),
        ),
        in_specs=[vmem] * 4 + [anywhere] * len(operands),
        out_specs=(vmem, vmem),
        scratch_shapes=[pltpu.VMEM(a.shape, a.dtype) for a in operands] + [
            pltpu.VMEM((4, merged), f32),
            pltpu.VMEM((rows, merged), f32),
            pltpu.VMEM((rows, merged), f32),
            pltpu.VMEM((rows, merged), f32),
            pltpu.VMEM((4, SUBLANES, merged), f32),
            pltpu.VMEM((n_ep, 4, merged), f32),
            pltpu.VMEM((n_tp, 2, rows // 2, channels), bf16),
            pltpu.VMEM((n_ep, 2, count // 2, features), bf16),
            pltpu.VMEM((n_ep, 2, count), jnp.int32),
            pltpu.VMEM((n_ep, 1, count), f32),
            pltpu.VMEM((2 * cap, features), bf16),
            pltpu.VMEM((n_ep, n_tp, 2, cap, ff // 2), bf16),
            pltpu.VMEM((n_ep, cap, columns), bf16),
            pltpu.VMEM((n_ep, cap, columns), bf16),
            pltpu.VMEM((n_tp, 2, count // 2, shared_ff), bf16),
            pltpu.VMEM((count, columns), f32),
            pltpu.VMEM((n_ep * cap, count), bf16),
            pltpu.VMEM((n_ep * cap, count), bf16),
            dma((len(operands),)), dma((n_ep, 2)), dma((1,)), dma((2,)), dma((1,)),
            dma((1,)), dma((2,)), dma((1,)), dma((1,)), dma((1,)), dma((4,)),
            dma((1,)), dma((n_ep, 4)), dma((1,)), dma((1,)), dma((1,)), dma((4,)),
        ],
        compiler_params=pltpu.CompilerParams(
            collective_id=0, has_side_effects=True, vmem_limit_bytes=56 * 1024 * 1024
        ),
        name="fused",
    )(
        routes.T, route_weight.T, log_step.reshape(1, groups), norm_gain.reshape(1, features),
        *operands,
    ))


def solution(mesh):
    placed = (
        P("ep", "tp"),
        P("tp"),
        P("ep", "tp"),
        P(None, "tp", None, None),
        P(None, "tp", None, None),
        P(None, "tp"),
        P("ep", None),
        P(),
        P("ep", None),
        P("ep", None),
        P("ep", None, "tp"),
        P("ep", None, "tp"),
        P("ep", None, "tp"),
        P(None, "tp"),
        P(None, "tp"),
        P(None, "tp"),
    )
    return jax.shard_map(
        shards,
        mesh=mesh,
        in_specs=placed,
        out_specs=(P("ep", "tp"), P("ep", "tp")),
        check_vma=False,
    )
```

```python
import functools
import math

import jax
import jax.numpy as jnp
from jax import lax
from jax.experimental import pallas as pl
from jax.experimental.pallas import tpu as pltpu
from jax.sharding import PartitionSpec as P

MESH = pl.DeviceIdType.MESH
SUBLANES = 8
NT = (((1,), (1,)), ((), ()))
TN = (((0,), (0,)), ((), ()))


def times(ar, ai, br, bi):
    return ar * br - ai * bi, ar * bi + ai * br


def iota(shape, dim):
    return lax.broadcasted_iota(jnp.int32, shape, dim)


def spread(shape, period):
    return (iota(shape, 1) % period == iota(shape, 0)).astype(jnp.bfloat16)


def halves(a):
    high = a.astype(jnp.bfloat16)
    return high, (a - high.astype(jnp.float32)).astype(jnp.bfloat16)


def dot(a, b, dims=None):
    if dims is None:
        return jnp.dot(a, b, preferred_element_type=jnp.float32)
    return lax.dot_general(a, b, dims, preferred_element_type=jnp.float32)


def fill_table(rate_ref, table, states):
    groups = rate_ref.shape[1]
    merged = table.shape[1]
    same = iota((groups, groups), 0) == iota((groups, groups), 1)
    column = jnp.sum(jnp.where(same, rate_ref[...], 0.0), axis=1, keepdims=True)
    place = iota((groups, merged), 1) // states == iota((groups, merged), 0)
    wide = jnp.sum(jnp.where(place, column, 0.0), axis=0, keepdims=True)
    step_rate = jnp.exp(wide)
    frequency = jnp.pi * lax.rem(iota((1, merged), 1), states).astype(jnp.float32)
    angle = step_rate * frequency
    turn_cosine = jnp.cos(angle)
    turn_sine = jnp.sin(angle)
    base = jnp.exp(-0.5 * step_rate)
    starting_quadrature = base * turn_sine
    inverse = 1.0 / (0.25 + frequency * frequency)
    lowered = base * turn_cosine - 1.0
    table[0:1, :] = turn_cosine
    table[1:2, :] = turn_sine
    table[2:3, :] = (-0.5 * lowered + starting_quadrature * frequency) * inverse
    table[3:4, :] = (-0.5 * starting_quadrature - lowered * frequency) * inverse
    return column


def drive_into(x_ref, column, shift_ref, map_ref, table_ref, mag, push_re, push_im, states):
    rows, channels = x_ref.shape
    merged = mag.shape[1]
    groups = shift_ref.shape[0]
    width = channels // groups
    steps = rows // SUBLANES
    place = iota((rows, rows), 0)
    order = (iota((rows, rows), 1) == (place % SUBLANES) * steps + place // SUBLANES).astype(
        jnp.bfloat16
    )
    level = jnp.exp(-0.5 * jnp.exp(column) + shift_ref[...])
    high, middle = halves(level)
    low = ((level - high.astype(jnp.float32)) - middle.astype(jnp.float32)).astype(jnp.bfloat16)
    widen = (iota((groups, merged), 1) // states == iota((groups, merged), 0)).astype(jnp.bfloat16)
    total = None
    for piece in (high, middle, low):
        part = dot(dot(order, piece, NT).astype(jnp.bfloat16), widen)
        total = part if total is None else total + part
    mag[...] = total
    x = dot(order, x_ref[...]).astype(jnp.bfloat16)
    repeat = spread((states, merged), states)
    mine = iota((channels, merged), 1) // states == iota((channels, merged), 0) // width
    drives = []
    for c in range(2):
        wide = jnp.where(mine, dot(map_ref[c], repeat), 0.0).astype(jnp.bfloat16)
        drives.append(dot(x, wide))
    re, im = times(table_ref[2:3, :], table_ref[3:4, :], drives[0], drives[1])
    push_re[...] = re
    push_im[...] = im


def sweep(table_ref, mag, push_re, push_im, start_re, start_im, keep):
    rows, merged = mag.shape
    turn_re = jnp.broadcast_to(table_ref[0:1, :], (SUBLANES, merged))
    turn_im = jnp.broadcast_to(table_ref[1:2, :], (SUBLANES, merged))

    def one(j, carry):
        re, im, product = carry
        at = pl.ds(pl.multiple_of(j * SUBLANES, SUBLANES), SUBLANES)
        level = mag[at, :]
        next_re, next_im = times(turn_re, turn_im, re, im)
        next_re = level * next_re + push_re[at, :]
        next_im = level * next_im + push_im[at, :]
        if keep:
            push_re[at, :] = next_re
            push_im[at, :] = next_im
        else:
            product = product * level
        return next_re, next_im, product

    product = jnp.ones((SUBLANES, merged), jnp.float32)
    if keep:
        def pair(j, carry):
            return one(j, carry + (None,))[:2]
        return lax.fori_loop(0, rows // SUBLANES, pair, (start_re, start_im))
    return lax.fori_loop(0, rows // SUBLANES, one, (start_re, start_im, product))


def power(wr, wi, steps):
    reached = 1
    while reached < steps:
        wr, wi = times(wr, wi, wr, wi)
        reached *= 2
    return wr, wi


def join(table_ref, ends_re, ends_im, product, pre, steps):
    merged = ends_re.shape[1]
    wr, wi = power(table_ref[0:1, :], table_ref[1:2, :], steps)
    cr = jnp.zeros((1, merged), jnp.float32)
    ci = cr
    ar = cr + 1.0
    ai = cr
    whole = cr + 1.0
    for s in range(SUBLANES):
        for i, v in enumerate((cr, ci, ar, ai)):
            pre[i, s : s + 1, :] = v
        level = product[s : s + 1]
        fr, fi = level * wr, level * wi
        tr, ti = times(fr, fi, cr, ci)
        cr, ci = tr + ends_re[s : s + 1], ti + ends_im[s : s + 1]
        ar, ai = times(fr, fi, ar, ai)
        whole = whole * level
    return cr, ci, whole


def follow(part, turn, re, im):
    re, im = times(turn[0], turn[1], re, im)
    return part[2:3] * re + part[0:1], part[2:3] * im + part[1:2]


def read_states(readout_ref, push_re, push_im, states):
    rows, merged = push_re.shape
    channels = readout_ref.shape[1]
    width = channels * states // merged
    repeat = spread((states, merged), states)
    mine = iota((channels, merged), 1) // states == iota((channels, merged), 0) // width
    total = None
    for c, ref in enumerate((push_re, push_im)):
        high, low = halves(ref[...])
        back = readout_ref[c] if c == 0 else -readout_ref[c]
        wide_high, wide_low = (
            jnp.where(mine, dot(half, repeat), 0.0).astype(jnp.bfloat16) for half in halves(back)
        )
        part = dot(high, wide_high, NT) + (dot(low, wide_high, NT) + dot(high, wide_low, NT))
        total = part if total is None else total + part
    place = iota((rows, rows), 0)
    steps = rows // SUBLANES
    order = (iota((rows, rows), 1) == (place % steps) * SUBLANES + place // steps).astype(
        jnp.bfloat16
    )
    cube = total + 0.044715 * (total * total * total)
    active = (0.5 * total * (1.0 + jnp.tanh(0.7978845608028654 * cube))).astype(jnp.bfloat16)
    return dot(order, active).astype(jnp.bfloat16)


def remote(src, dst, send, recv, **target):
    return pltpu.make_async_remote_copy(
        src_ref=src, dst_ref=dst, send_sem=send, recv_sem=recv,
        device_id=target, device_id_type=MESH,
    )


def visits(chips):
    plan = []
    for chip in range(chips):
        end = chip in (0, chips - 1)
        found = []
        for d in range(1, chips):
            for j in range(2):
                for there, onward in ((chip - d, chip + 1), (chip + d, chip - 1)):
                    if 0 <= there < chips:
                        onward = onward if 0 <= onward < chips else -1
                        found.append((2 * there + j, onward, 2 * d + j))
        units = []
        for u, (source, onward, arrival) in enumerate(found):
            together = max(v for v in range(len(found)) if found[v][2] == arrival)
            ahead = max((3 * together - 1) // 2, 3 * together - 7) if together > 1 else 0
            units.append((source, onward, 3 * u if end else ahead))
        plan.append(units)
    return plan


def fused_kernel(
    n_ep, n_tp, states,
    routes_ref, gains_ref, rate_ref, gain_ref,
    input_hbm, x_hbm, shift_hbm, map_hbm, readout_hbm, weight_hbm,
    sgate_hbm, sup_hbm, sdown_hbm, gate_hbm, up_hbm, down_hbm,
    out_ref, experts_ref,
    tokens, x_ref, shift_ref, map_ref, readout_ref, weight_ref,
    sgate, sup, sdown, gate, up, down,
    table, mag, push_re, push_im, pre, blocks, summary, active,
    tok, named, ranks, picked, hidden, result, returned, shared, common, high, low,
    load, tok_recv, mate_send, own_send, on_send, n_send, n_recv,
    b_send, b_recv, e_send, e_recv, a_send, a_recv, h_send, h_recv, r_send, r_recv, s_send, s_recv,
):
    ep = lax.axis_index("ep")
    tp = lax.axis_index("tp")
    rows, channels = x_ref.shape
    merged = mag.shape[1]
    half_rows, features = tok.shape[2:]
    count = 2 * half_rows
    cap = picked.shape[0] // 2
    chips = n_ep // 2
    chip, core = ep // 2, lax.rem(ep, 2)
    mate = ep + 1 - 2 * core
    side = math.isqrt(n_tp)
    y, x = tp // side, lax.rem(tp, side)
    pieces, quarter = hidden.shape[2], hidden.shape[4]
    half = 2 * quarter

    first_load = pltpu.make_async_copy(input_hbm, tokens, load.at[0])
    first_load.start()
    barrier = pltpu.get_barrier_semaphore()
    for d in range(1, n_ep):
        pl.semaphore_signal(
            barrier, inc=1, device_id={"ep": lax.rem(ep + d, n_ep)}, device_id_type=MESH
        )
    for d in range(1, n_tp):
        pl.semaphore_signal(
            barrier, inc=1, device_id={"tp": lax.rem(tp + d, n_tp)}, device_id_type=MESH
        )
    pairs = (
        (input_hbm, tokens), (sgate_hbm, sgate), (sup_hbm, sup), (gate_hbm, gate), (up_hbm, up),
        (x_hbm, x_ref), (shift_hbm, shift_ref), (map_hbm, map_ref), (down_hbm, down),
        (readout_hbm, readout_ref), (weight_hbm, weight_ref), (sdown_hbm, sdown),
    )
    loads = [pltpu.make_async_copy(a, b, load.at[i]) for i, (a, b) in enumerate(pairs)]
    for copy in loads[1:]:
        copy.start()
    def across(dy, dx):
        return lax.rem(y + dy, side) * side + lax.rem(x + dx, side)

    peers = {(dy, dx): across(dy, dx) for dy in range(side) for dx in range(side)}

    class Share:
        def __init__(self, buffer, send, recv):
            self.buffer, self.send, self.recv = buffer, send, recv
            self.pieces = buffer.shape[1]

        def copy(self, source, h, to, k):
            at = self.buffer.at[source, h]
            return remote(at, at, self.send, self.recv.at[k], tp=to)

        def start(self, h):
            for first in (True, False):
                for o in range(1, side):
                    row, column = (h, h + 1) if first else (h + 1, h)
                    k = h // 2 if first else self.pieces // 2
                    self.copy(tp, row, peers[0, o], k).start()
                    self.copy(tp, column, peers[o, 0], k).start()

        def wait(self, at, k):
            remote(at, at, self.send, self.recv.at[k], tp=peers[0, 1]).wait_recv()

        def forward(self):
            far = self.pieces // 2 + 1
            for h in range(0, self.pieces, 2):
                self.wait(self.buffer.at[pl.ds(0, side - 1), pl.ds(h, 2)], h // 2)
                for o in range(1, side):
                    for d in range(1, side):
                        self.copy(peers[0, o], h, peers[d, 0], far).start()
                        self.copy(peers[o, 0], h + 1, peers[0, d], far).start()

        def near(self):
            self.wait(self.buffer.at[pl.ds(0, side - 1)], self.pieces // 2)

        def far(self):
            self.wait(self.buffer.at[pl.ds(0, (side - 1) ** 2)], self.pieces // 2 + 1)

        def drain(self, at):
            remote(at, at, self.send, self.recv.at[0], tp=peers[0, 1]).wait_send()

    def hidden_of(s):
        return Share(hidden.at[s], h_send.at[0], h_recv.at[s])

    shared_out = Share(shared, s_send.at[0], s_recv)
    active_out = Share(active, a_send.at[0], a_recv)

    first_load.wait()
    block = 16
    scale = gain_ref[...]

    @pl.loop(0, half_rows // block)
    def _(i):
        at = pl.ds(pl.multiple_of(i * block, block), block)
        for h in range(2):
            values = tokens[h, at, :].astype(jnp.float32)
            level = lax.rsqrt(jnp.mean(values * values, axis=-1, keepdims=True) + 1e-06)
            tok[ep, h, at, :] = (values * level * scale).astype(jnp.bfloat16)

    named[ep] = routes_ref[...]
    pl.semaphore_wait(barrier, n_ep + n_tp - 2)

    def piece(s, h, send, target):
        return remote(tok.at[s, h], tok.at[s, h], send, tok_recv.at[s, h], ep=target)

    piece(ep, 1 - core, mate_send.at[0], mate).start()
    piece(ep, core, mate_send.at[0], mate).start()
    remote(routes_ref, named.at[ep], n_send.at[0], n_recv.at[0], ep=mate).start()
    strangers = [
        2 * lax.rem(chip + d, chips) + c for d in range(1, chips) for c in range(2)
    ]
    for target in strangers:
        remote(routes_ref, named.at[ep], n_send.at[0], n_recv.at[1], ep=target).start()
    ends = ((chip > 0, lax.rem(ep + n_ep - 2, n_ep)), (chip < chips - 1, lax.rem(ep + 2, n_ep)))

    def own(j, d):
        return piece(2 * chip + j, core, own_send.at[d], ends[d][1])

    def depart(j):
        @pl.when(core != j)
        def _():
            piece(2 * chip + j, core, mate_send.at[0], mate).wait_recv()

        for d in range(2):
            @pl.when(ends[d][0])
            def _():
                own(j, d).start()

    depart(0)

    def shared_hidden():
        for copy in loads[1:3]:
            copy.wait()
        a = tok[ep].reshape(count, features)
        v = dot(a, sgate[...])
        shared[tp] = (v / (1.0 + jnp.exp(-v)) * dot(a, sup[...])).astype(jnp.bfloat16).reshape(
            shared.shape[1:]
        )
        shared_out.start(0)

    later = (iota((count, count), 0) <= iota((count, count), 1)).astype(jnp.bfloat16)
    slots = iota((cap, count), 0).astype(jnp.float32)

    def member(names, expert):
        return jnp.where(jnp.logical_or(names[0:1] == expert, names[1:2] == expert), 1.0, 0.0)

    def seats(mine):
        return jnp.where(mine > 0.0, dot(mine.astype(jnp.bfloat16), later) - 1.0, -1.0)

    def process(*group):
        for i, s in enumerate(group):
            chosen = (slots == ranks[s]).astype(jnp.bfloat16)
            picked[i * cap : (i + 1) * cap, :] = dot(
                chosen, tok[s].reshape(count, features)
            ).astype(jnp.bfloat16)
        a = picked[: len(group) * cap, :]
        for h in range(0, pieces, 2):
            at = slice(h * quarter, h * quarter + half)
            v = dot(a, gate[:, at])
            v = (v / (1.0 + jnp.exp(-v)) * dot(a, up[:, at])).astype(jnp.bfloat16)
            for i, s in enumerate(group):
                for k in range(2):
                    hidden[s, tp, h + k] = v[
                        i * cap : (i + 1) * cap, k * quarter : (k + 1) * quarter
                    ]
                hidden_of(s).start(h)

    def back(s):
        return remote(result.at[s], returned.at[ep], r_send.at[0], r_recv.at[0], ep=s)

    def project(*group, now=True):
        def part(q):
            total = None
            for h in range(pieces):
                a = jnp.concatenate([hidden[s, q, h] for s in group], axis=0)
                one = dot(a, down[q, h])
                total = one if total is None else total + one
            return total

        total = part(tp)
        for s in group:
            hidden_of(s).near()
        for o in range(1, side):
            total = total + part(peers[0, o])
            total = total + part(peers[o, 0])
        for s in group:
            hidden_of(s).far()
        for dy in range(1, side):
            for dx in range(1, side):
                total = total + part(peers[dy, dx])
        for i, s in enumerate(group):
            result[s] = total[i * cap : (i + 1) * cap].astype(jnp.bfloat16)
        if len(group) == 2:
            returned[ep] = result[ep]
            back(mate).start()
        elif now:
            back(group[0]).start()

    def scan_block():
        for copy in loads[5:8]:
            copy.wait()
        column = fill_table(rate_ref, table, states)
        drive_into(x_ref, column, shift_ref, map_ref, table, mag, push_re, push_im, states)
        zero = jnp.zeros((SUBLANES, merged), jnp.float32)
        ends_re, ends_im, product = sweep(table, mag, push_re, push_im, zero, zero, False)
        end = join(table, ends_re, ends_im, product, pre, rows // SUBLANES)
        for i, v in enumerate(end):
            blocks[core, i : i + 1, :] = v

        @pl.when(core == 0)
        def _():
            first_block().start()

    def first_block():
        return remote(blocks.at[0], blocks.at[0], b_send.at[0], b_recv.at[0], ep=mate)

    def whole_chip(d, c):
        return remote(
            summary.at[chip], summary.at[chip], e_send.at[d], e_recv.at[chip],
            ep=lax.rem(2 * (chip + d) + c, n_ep),
        )

    def turn_over(count):
        return power(table[0:1, :], table[1:2, :], count)

    def scan_chip():
        @pl.when(core == 1)
        def _():
            first_block().wait_recv()
            first = blocks[0]
            part = blocks[1]
            re, im = follow(part, turn_over(rows), first[0:1], first[1:2])
            for i, v in enumerate((re, im, first[2:3] * part[2:3])):
                summary[chip, i : i + 1, :] = v
            for d in range(1, chips):
                @pl.when(chip + d < chips)
                def _():
                    for c in range(2):
                        whole_chip(d, c).start()

    def rank(first, number):
        mine = [member(named[first + i], ep) for i in range(number)]
        mine += [mine[0]] * (-number % SUBLANES)
        place = seats(jnp.concatenate(mine, axis=0))
        for i in range(number):
            ranks[first + i] = place[i : i + 1]

    def gain_blocks():
        names = routes_ref[...]
        level = gains_ref[...]
        wanted = [member(names, e) for e in range(n_ep)]
        wanted += [wanted[0]] * (-n_ep % SUBLANES)
        places = seats(jnp.concatenate(wanted, axis=0))
        for e in range(n_ep):
            weight = jnp.where(names[0:1] == e, level[0:1], 0.0) + jnp.where(
                names[1:2] == e, level[1:2], 0.0
            )
            wide = jnp.where(slots == places[e : e + 1], weight, 0.0)
            top, rest = halves(wide)
            high[e * cap : (e + 1) * cap, :] = top
            low[e * cap : (e + 1) * cap, :] = rest

    def scan_states():
        for k in range(chips - 1):
            @pl.when(k < chip)
            def _():
                remote(
                    summary.at[k], summary.at[k], e_send.at[0], e_recv.at[k], ep=mate
                ).wait_recv()

        turn = turn_over(2 * rows)

        def fold(k, carry):
            return follow(summary[k], turn, *carry)

        nothing = jnp.zeros((1, merged), jnp.float32)
        in_re, in_im = lax.fori_loop(0, chip, fold, (nothing, nothing))
        step_re, step_im = follow(blocks[0], turn_over(rows), in_re, in_im)
        in_re = jnp.where(core == 1, step_re, in_re)
        in_im = jnp.where(core == 1, step_im, in_im)
        add_re, add_im = times(pre[2], pre[3], in_re, in_im)
        sweep(table, mag, push_re, push_im, pre[0] + add_re, pre[1] + add_im, True)
        loads[9].wait()
        active[tp] = read_states(readout_ref, push_re, push_im, states).reshape(active.shape[1:])
        active_out.start(0)

    def mix():
        active_out.near()
        active_out.far()
        loads[10].wait()
        total = None
        for q in range(n_tp):
            a = active[q].reshape(rows, channels)
            part = dot(a, weight_ref[q * channels : (q + 1) * channels, :])
            total = part if total is None else total + part
        out_ref[...] = total.astype(out_ref.dtype)
        shared_out.near()
        shared_out.far()
        loads[11].wait()
        width = shared.shape[3]
        total = None
        for q in range(n_tp):
            a = shared[q].reshape(count, width)
            part = dot(a, sdown[q * width : (q + 1) * width, :])
            total = part if total is None else total + part
        common[...] = total

    plan = visits(chips)
    last = len(plan[0]) - 1

    def here(u, field):
        value = jnp.int32(plan[0][u][field])
        for k in range(1, chips):
            value = jnp.where(chip == k, jnp.int32(plan[k][u][field]), value)
        return value

    source = [here(u, 0) for u in range(last + 1)]
    onward = [here(u, 1) for u in range(last + 1)]
    steps = [here(u, 2) for u in range(last + 1)]

    def along(u):
        target = 2 * jnp.maximum(onward[u], 0) + core
        return piece(source[u], core, on_send.at[0], target)

    def aside(u):
        return piece(source[u], core, mate_send.at[0], mate)

    def pass_on(u):
        aside(u).wait_recv()

        @pl.when(onward[u] >= 0)
        def _():
            along(u).start()

        aside(u).start()

    def ready(s):
        piece(s, 1 - core, mate_send.at[0], mate).wait_recv()

    groups = [(2 * chip, 2 * chip + 1)] + [(s,) for s in source]

    def forward(group):
        for s in group:
            hidden_of(s).forward()

    shared_hidden()
    depart(1)
    for copy in loads[3:5]:
        copy.wait()
    ready(mate)
    remote(routes_ref, named.at[mate], n_send.at[0], n_recv.at[0], ep=mate).wait_recv()
    rank(2 * chip, 2)
    process(*groups[0])
    scan_block()
    gain_blocks()
    scan_chip()
    shared_out.forward()
    rest = named.at[pl.ds(0, n_ep - 2)]
    remote(rest, rest, n_send.at[0], n_recv.at[1], ep=mate).wait_recv()
    rank(0, n_ep)

    def arrivals(step):
        for v in range(last + 1):
            if any(units[v][2] == step for units in plan):
                @pl.when(steps[v] == step)
                def _():
                    pass_on(v)

    for u in range(last + 1):
        arrivals(3 * u)
        if u == last:
            forward(groups[u])
        ready(source[u])
        process(source[u])
        arrivals(3 * u + 1)
        if u == min(1, last):
            scan_states()
        if u < last:
            forward(groups[u])
        if u == min(2, last):
            active_out.forward()
        if u == 1:
            loads[8].wait()
        if u > 0:
            project(*groups[u - 1], now=u != 2)
        arrivals(3 * u + 2)
        if u == 2:
            back(source[0]).start()
        if u == min(4, last):
            mix()
    project(*groups[last])
    forward(groups[last + 1])
    project(*groups[last + 1])
    rest = returned.at[pl.ds(0, n_ep - 1)]
    remote(rest, rest, r_send.at[0], r_recv.at[0], ep=mate).wait_recv()
    back_rows = returned[...].reshape(n_ep * cap, returned.shape[2])
    routed = dot(high[...], back_rows, TN) + dot(low[...], back_rows, TN)
    experts_ref[...] = (common[...] + routed).astype(experts_ref.dtype)
    shared_out.drain(shared.at[pl.ds(0, n_tp - 1)])
    active_out.drain(active.at[pl.ds(0, n_tp - 1)])
    hidden_of(ep).drain(hidden.at[:, pl.ds(0, n_tp - 1)])

    def drain(at, send, recv):
        remote(at, at, send, recv, ep=mate).wait_send()

    drain(named.at[pl.ds(0, n_ep - 1)], n_send.at[0], n_recv.at[0])

    @pl.when(core == 0)
    def _():
        first_block().wait_send()

    for d in range(1, chips):
        @pl.when(jnp.logical_and(core == 1, chip + d < chips))
        def _():
            drain(summary.at[pl.ds(0, 2)], e_send.at[d], e_recv.at[0])

    drain(result.at[pl.ds(0, n_ep - 1)], r_send.at[0], r_recv.at[0])
    drain(tok.at[:, 0], mate_send.at[0], tok_recv.at[0, 0])
    for d in range(2):
        @pl.when(ends[d][0])
        def _():
            drain(tok.at[pl.ds(0, 2), 0], own_send.at[d], tok_recv.at[0, 0])

    @pl.when(jnp.logical_and(ends[0][0], ends[1][0]))
    def _():
        drain(tok.at[pl.ds(0, last + 1), 0], on_send.at[0], tok_recv.at[0, 0])


def shards(
    mixer_input,
    log_step,
    decay_shift,
    input_map,
    readout,
    mixer_weight,
    expert_input,
    norm_gain,
    routes,
    route_weight,
    expert_switch_matrix,
    up_weight,
    down_weight,
    shared_gate,
    shared_up,
    shared_down,
):
    n_ep, n_tp = lax.axis_size("ep"), lax.axis_size("tp")
    count, features = expert_input.shape
    cap = 2 * count * routes.shape[1] // n_ep
    rows, channels = mixer_input.shape
    groups = log_step.shape[0]
    states, width = input_map.shape[2:]
    merged = groups * states
    f32, bf16 = jnp.float32, jnp.bfloat16
    ff = up_weight.shape[2]
    depth, columns = down_weight.shape[1:]
    shared_ff = shared_up.shape[1]
    vmem = pl.BlockSpec(memory_space=pltpu.VMEM)
    anywhere = pl.BlockSpec(memory_space=pl.ANY)
    dma = pltpu.SemaphoreType.DMA
    operands = (
        expert_input.reshape(2, count // 2, features),
        mixer_input,
        decay_shift.T,
        input_map.swapaxes(2, 3).reshape(2, channels, states),
        readout.reshape(2, channels, states),
        mixer_weight,
        shared_gate,
        shared_up,
        shared_down,
        expert_switch_matrix.reshape(features, ff),
        up_weight.reshape(features, ff),
        down_weight.reshape(n_tp, 4, ff // 4, columns),
    )
    return tuple(pl.pallas_call(
        functools.partial(fused_kernel, n_ep, n_tp, states),
        out_shape=(
            pltpu.VMEM((rows, mixer_weight.shape[1]), bf16),
            pltpu.VMEM((count, columns), bf16),
        ),
        in_specs=[vmem] * 4 + [anywhere] * len(operands),
        out_specs=(vmem, vmem),
        scratch_shapes=[pltpu.VMEM(a.shape, a.dtype) for a in operands] + [
            pltpu.VMEM((4, merged), f32),
            pltpu.VMEM((rows, merged), f32),
            pltpu.VMEM((rows, merged), f32),
            pltpu.VMEM((rows, merged), f32),
            pltpu.VMEM((4, SUBLANES, merged), f32),
            pltpu.VMEM((2, 3, merged), f32),
            pltpu.VMEM((n_ep // 2, 3, merged), f32),
            pltpu.VMEM((n_tp, 2, rows // 2, channels), bf16),
            pltpu.VMEM((n_ep, 2, count // 2, features), bf16),
            pltpu.VMEM((n_ep, 2, count), jnp.int32),
            pltpu.VMEM((n_ep, 1, count), f32),
            pltpu.VMEM((2 * cap, features), bf16),
            pltpu.VMEM((n_ep, n_tp, 4, cap, ff // 4), bf16),
            pltpu.VMEM((n_ep, cap, columns), bf16),
            pltpu.VMEM((n_ep, cap, columns), bf16),
            pltpu.VMEM((n_tp, 2, count // 2, shared_ff), bf16),
            pltpu.VMEM((count, columns), f32),
            pltpu.VMEM((n_ep * cap, count), bf16),
            pltpu.VMEM((n_ep * cap, count), bf16),
            dma((len(operands),)), dma((n_ep, 2)), dma((1,)), dma((2,)), dma((1,)),
            dma((1,)), dma((2,)), dma((1,)), dma((1,)), dma((n_ep // 2,)), dma((n_ep // 2,)),
            dma((1,)), dma((3,)),
            dma((1,)), dma((n_ep, 4)), dma((1,)), dma((1,)), dma((1,)), dma((3,)),
        ],
        compiler_params=pltpu.CompilerParams(
            collective_id=0, has_side_effects=True, vmem_limit_bytes=56 * 1024 * 1024
        ),
        name="fused",
    )(
        routes.T, route_weight.T, log_step.reshape(1, groups), norm_gain.reshape(1, features),
        *operands,
    ))


def solution(mesh):
    placed = (
        P("ep", "tp"),
        P("tp"),
        P("ep", "tp"),
        P(None, "tp", None, None),
        P(None, "tp", None, None),
        P(None, "tp"),
        P("ep", None),
        P(),
        P("ep", None),
        P("ep", None),
        P("ep", None, "tp"),
        P("ep", None, "tp"),
        P("ep", None, "tp"),
        P(None, "tp"),
        P(None, "tp"),
        P(None, "tp"),
    )
    return jax.shard_map(
        shards,
        mesh=mesh,
        in_specs=placed,
        out_specs=(P("ep", "tp"), P("ep", "tp")),
        check_vma=False,
    )
```

```python
import functools
import math

import jax
import jax.numpy as jnp
from jax import lax
from jax.experimental import pallas as pl
from jax.experimental.pallas import tpu as pltpu
from jax.sharding import PartitionSpec as P

MESH = pl.DeviceIdType.MESH
SUBLANES = 8
NT = (((1,), (1,)), ((), ()))
TN = (((0,), (0,)), ((), ()))


def times(ar, ai, br, bi):
    return ar * br - ai * bi, ar * bi + ai * br


def iota(shape, dim):
    return lax.broadcasted_iota(jnp.int32, shape, dim)


def spread(shape, period):
    return (iota(shape, 1) % period == iota(shape, 0)).astype(jnp.bfloat16)


def halves(a):
    high = a.astype(jnp.bfloat16)
    return high, (a - high.astype(jnp.float32)).astype(jnp.bfloat16)


def dot(a, b, dims=None):
    if dims is None:
        return jnp.dot(a, b, preferred_element_type=jnp.float32)
    return lax.dot_general(a, b, dims, preferred_element_type=jnp.float32)


def fill_table(rate_ref, table, states):
    groups = rate_ref.shape[1]
    merged = table.shape[1]
    same = iota((groups, groups), 0) == iota((groups, groups), 1)
    column = jnp.sum(jnp.where(same, rate_ref[...], 0.0), axis=1, keepdims=True)
    place = iota((groups, merged), 1) // states == iota((groups, merged), 0)
    wide = jnp.sum(jnp.where(place, column, 0.0), axis=0, keepdims=True)
    step_rate = jnp.exp(wide)
    frequency = jnp.pi * lax.rem(iota((1, merged), 1), states).astype(jnp.float32)
    angle = step_rate * frequency
    turn_cosine = jnp.cos(angle)
    turn_sine = jnp.sin(angle)
    base = jnp.exp(-0.5 * step_rate)
    starting_quadrature = base * turn_sine
    inverse = 1.0 / (0.25 + frequency * frequency)
    lowered = base * turn_cosine - 1.0
    table[0:1, :] = turn_cosine
    table[1:2, :] = turn_sine
    table[2:3, :] = (-0.5 * lowered + starting_quadrature * frequency) * inverse
    table[3:4, :] = (-0.5 * starting_quadrature - lowered * frequency) * inverse
    return column


def drive_into(x_ref, column, shift_ref, map_ref, table_ref, mag, push_re, push_im, states):
    rows, channels = x_ref.shape
    merged = mag.shape[1]
    groups = shift_ref.shape[0]
    width = channels // groups
    steps = rows // SUBLANES
    place = iota((rows, rows), 0)
    order = (iota((rows, rows), 1) == (place % SUBLANES) * steps + place // SUBLANES).astype(
        jnp.bfloat16
    )
    level = jnp.exp(-0.5 * jnp.exp(column) + shift_ref[...])
    high, middle = halves(level)
    low = ((level - high.astype(jnp.float32)) - middle.astype(jnp.float32)).astype(jnp.bfloat16)
    widen = (iota((groups, merged), 1) // states == iota((groups, merged), 0)).astype(jnp.bfloat16)
    total = None
    for piece in (high, middle, low):
        part = dot(dot(order, piece, NT).astype(jnp.bfloat16), widen)
        total = part if total is None else total + part
    mag[...] = total
    x = dot(order, x_ref[...]).astype(jnp.bfloat16)
    repeat = spread((states, merged), states)
    mine = iota((channels, merged), 1) // states == iota((channels, merged), 0) // width
    drives = []
    for c in range(2):
        wide = jnp.where(mine, dot(map_ref[c], repeat), 0.0).astype(jnp.bfloat16)
        drives.append(dot(x, wide))
    re, im = times(table_ref[2:3, :], table_ref[3:4, :], drives[0], drives[1])
    push_re[...] = re
    push_im[...] = im


def sweep(table_ref, mag, push_re, push_im, start_re, start_im, keep):
    rows, merged = mag.shape
    turn_re = jnp.broadcast_to(table_ref[0:1, :], (SUBLANES, merged))
    turn_im = jnp.broadcast_to(table_ref[1:2, :], (SUBLANES, merged))

    def one(j, carry):
        re, im, product = carry
        at = pl.ds(pl.multiple_of(j * SUBLANES, SUBLANES), SUBLANES)
        level = mag[at, :]
        next_re, next_im = times(turn_re, turn_im, re, im)
        next_re = level * next_re + push_re[at, :]
        next_im = level * next_im + push_im[at, :]
        if keep:
            push_re[at, :] = next_re
            push_im[at, :] = next_im
        else:
            product = product * level
        return next_re, next_im, product

    product = jnp.ones((SUBLANES, merged), jnp.float32)
    if keep:
        def pair(j, carry):
            return one(j, carry + (None,))[:2]
        return lax.fori_loop(0, rows // SUBLANES, pair, (start_re, start_im))
    return lax.fori_loop(0, rows // SUBLANES, one, (start_re, start_im, product))


def power(wr, wi, steps):
    reached = 1
    while reached < steps:
        wr, wi = times(wr, wi, wr, wi)
        reached *= 2
    return wr, wi


def join(table_ref, ends_re, ends_im, product, pre, steps):
    merged = ends_re.shape[1]
    wr, wi = power(table_ref[0:1, :], table_ref[1:2, :], steps)
    cr = jnp.zeros((1, merged), jnp.float32)
    ci = cr
    ar = cr + 1.0
    ai = cr
    whole = cr + 1.0
    for s in range(SUBLANES):
        for i, v in enumerate((cr, ci, ar, ai)):
            pre[i, s : s + 1, :] = v
        level = product[s : s + 1]
        fr, fi = level * wr, level * wi
        tr, ti = times(fr, fi, cr, ci)
        cr, ci = tr + ends_re[s : s + 1], ti + ends_im[s : s + 1]
        ar, ai = times(fr, fi, ar, ai)
        whole = whole * level
    return cr, ci, whole


def follow(part, turn, re, im):
    re, im = times(turn[0], turn[1], re, im)
    return part[2:3] * re + part[0:1], part[2:3] * im + part[1:2]


def read_states(readout_ref, push_re, push_im, states):
    rows, merged = push_re.shape
    channels = readout_ref.shape[1]
    width = channels * states // merged
    repeat = spread((states, merged), states)
    mine = iota((channels, merged), 1) // states == iota((channels, merged), 0) // width
    total = None
    for c, ref in enumerate((push_re, push_im)):
        high, low = halves(ref[...])
        back = readout_ref[c] if c == 0 else -readout_ref[c]
        wide_high, wide_low = (
            jnp.where(mine, dot(half, repeat), 0.0).astype(jnp.bfloat16) for half in halves(back)
        )
        part = dot(high, wide_high, NT) + (dot(low, wide_high, NT) + dot(high, wide_low, NT))
        total = part if total is None else total + part
    place = iota((rows, rows), 0)
    steps = rows // SUBLANES
    order = (iota((rows, rows), 1) == (place % steps) * SUBLANES + place // steps).astype(
        jnp.bfloat16
    )
    cube = total + 0.044715 * (total * total * total)
    active = (0.5 * total * (1.0 + jnp.tanh(0.7978845608028654 * cube))).astype(jnp.bfloat16)
    return dot(order, active).astype(jnp.bfloat16)


def remote(src, dst, send, recv, **target):
    return pltpu.make_async_remote_copy(
        src_ref=src, dst_ref=dst, send_sem=send, recv_sem=recv,
        device_id=target, device_id_type=MESH,
    )


def visits(chips):
    plan = []
    for chip in range(chips):
        end = chip in (0, chips - 1)
        found = []
        for d in range(1, chips):
            for j in range(2):
                for there, onward in ((chip - d, chip + 1), (chip + d, chip - 1)):
                    if 0 <= there < chips:
                        onward = onward if 0 <= onward < chips else -1
                        found.append((2 * there + j, onward, 2 * d + j))
        units = []
        for u, (source, onward, arrival) in enumerate(found):
            together = max(v for v in range(len(found)) if found[v][2] == arrival)
            ahead = max((3 * together - 1) // 2, 3 * together - 7) if together > 1 else 0
            units.append((source, onward, 3 * u if end else ahead))
        plan.append(units)
    return plan


def fused_kernel(
    n_ep, n_tp, states,
    routes_hbm, gains_hbm, rate_hbm, gain_hbm, input_hbm, x_hbm, shift_hbm, map_hbm, readout_hbm, weight_hbm,
    sgate_hbm, sup_hbm, sdown_hbm, gate_hbm, up_hbm, down_hbm,
    out_ref, experts_ref,
    routes_ref, gains_ref, rate_ref, gain_ref, tokens, x_ref, shift_ref, map_ref, readout_ref, weight_ref,
    sgate, sup, sdown, gate, up, down,
    table, mag, push_re, push_im, pre, blocks, summary, active,
    tok, named, ranks, picked, hidden, result, returned, shared, common, high, low,
    load, tok_recv, mate_send, own_send, on_send, n_send, n_recv,
    b_send, b_recv, e_send, e_recv, a_send, a_recv, h_send, h_recv, r_send, r_recv, s_send, s_recv,
):
    ep = lax.axis_index("ep")
    tp = lax.axis_index("tp")
    rows, channels = x_ref.shape
    merged = mag.shape[1]
    half_rows, features = tok.shape[2:]
    count = 2 * half_rows
    cap = picked.shape[0] // 2
    chips = n_ep // 2
    chip, core = ep // 2, lax.rem(ep, 2)
    mate = ep + 1 - 2 * core
    side = math.isqrt(n_tp)
    y, x = tp // side, lax.rem(tp, side)
    pieces, quarter = hidden.shape[2], hidden.shape[4]
    half = 2 * quarter

    first_loads = [
        pltpu.make_async_copy(a, b, load.at[i])
        for i, (a, b) in enumerate((
            (input_hbm, tokens), (gain_hbm, gain_ref), (routes_hbm, routes_ref),
            (gains_hbm, gains_ref), (rate_hbm, rate_ref),
        ))
    ]
    for copy in first_loads:
        copy.start()
    barrier = pltpu.get_barrier_semaphore()
    for d in range(1, n_ep):
        pl.semaphore_signal(
            barrier, inc=1, device_id={"ep": lax.rem(ep + d, n_ep)}, device_id_type=MESH
        )
    for d in range(1, n_tp):
        pl.semaphore_signal(
            barrier, inc=1, device_id={"tp": lax.rem(tp + d, n_tp)}, device_id_type=MESH
        )
    pairs = (
        (sgate_hbm, sgate), (sup_hbm, sup), (gate_hbm, gate), (up_hbm, up),
        (x_hbm, x_ref), (shift_hbm, shift_ref), (map_hbm, map_ref), (down_hbm, down),
        (readout_hbm, readout_ref), (weight_hbm, weight_ref), (sdown_hbm, sdown),
    )
    loads = [
        pltpu.make_async_copy(a, b, load.at[len(first_loads) + i])
        for i, (a, b) in enumerate(pairs)
    ]
    for copy in loads:
        copy.start()
    def across(dy, dx):
        return lax.rem(y + dy, side) * side + lax.rem(x + dx, side)

    peers = {(dy, dx): across(dy, dx) for dy in range(side) for dx in range(side)}

    class Share:
        def __init__(self, buffer, send, recv):
            self.buffer, self.send, self.recv = buffer, send, recv
            self.pieces = buffer.shape[1]

        def copy(self, source, h, to, k):
            at = self.buffer.at[source, h]
            return remote(at, at, self.send, self.recv.at[k], tp=to)

        def start(self, h):
            for o in range(1, side):
                self.copy(tp, h, peers[0, o], h // 2).start()
                self.copy(tp, h + 1, peers[o, 0], h // 2).start()
            if h + 2 == self.pieces:
                for g in range(0, self.pieces, 2):
                    for o in range(1, side):
                        self.copy(tp, g + 1, peers[0, o], self.pieces // 2).start()
                        self.copy(tp, g, peers[o, 0], self.pieces // 2).start()

        def wait(self, at, k):
            remote(at, at, self.send, self.recv.at[k], tp=peers[0, 1]).wait_recv()

        def forward(self):
            far = self.pieces // 2 + 1
            for h in range(0, self.pieces, 2):
                self.wait(self.buffer.at[pl.ds(0, side - 1), pl.ds(h, 2)], h // 2)
                for o in range(1, side):
                    for d in range(1, side):
                        self.copy(peers[0, o], h, peers[d, 0], far).start()
                        self.copy(peers[o, 0], h + 1, peers[0, d], far).start()

        def near(self):
            self.wait(self.buffer.at[pl.ds(0, side - 1)], self.pieces // 2)

        def far(self):
            self.wait(self.buffer.at[pl.ds(0, (side - 1) ** 2)], self.pieces // 2 + 1)

        def drain(self, at):
            remote(at, at, self.send, self.recv.at[0], tp=peers[0, 1]).wait_send()

    def hidden_of(s):
        return Share(hidden.at[s], h_send.at[0], h_recv.at[s])

    shared_out = Share(shared, s_send.at[0], s_recv)
    active_out = Share(active, a_send.at[0], a_recv)

    for copy in first_loads:
        copy.wait()
    block = 16
    scale = gain_ref[...]

    @pl.loop(0, half_rows // block)
    def _(i):
        at = pl.ds(pl.multiple_of(i * block, block), block)
        for h in range(2):
            values = tokens[h, at, :].astype(jnp.float32)
            level = lax.rsqrt(jnp.mean(values * values, axis=-1, keepdims=True) + 1e-06)
            tok[ep, h, at, :] = (values * level * scale).astype(jnp.bfloat16)

    named[ep] = routes_ref[...]
    pl.semaphore_wait(barrier, n_ep + n_tp - 2)

    def piece(s, h, send, target):
        return remote(tok.at[s, h], tok.at[s, h], send, tok_recv.at[s, h], ep=target)

    piece(ep, 1 - core, mate_send.at[0], mate).start()
    piece(ep, core, mate_send.at[0], mate).start()
    remote(routes_ref, named.at[ep], n_send.at[0], n_recv.at[0], ep=mate).start()
    strangers = [
        2 * lax.rem(chip + d, chips) + c for d in range(1, chips) for c in range(2)
    ]
    for target in strangers:
        remote(routes_ref, named.at[ep], n_send.at[0], n_recv.at[1], ep=target).start()
    ends = ((chip > 0, lax.rem(ep + n_ep - 2, n_ep)), (chip < chips - 1, lax.rem(ep + 2, n_ep)))

    def own(j, d):
        return piece(2 * chip + j, core, own_send.at[d], ends[d][1])

    def depart(j):
        @pl.when(core != j)
        def _():
            piece(2 * chip + j, core, mate_send.at[0], mate).wait_recv()

        for d in range(2):
            @pl.when(ends[d][0])
            def _():
                own(j, d).start()

    depart(0)

    def shared_hidden():
        for copy in loads[0:2]:
            copy.wait()
        a = tok[ep].reshape(count, features)
        v = dot(a, sgate[...])
        shared[tp] = (v / (1.0 + jnp.exp(-v)) * dot(a, sup[...])).astype(jnp.bfloat16).reshape(
            shared.shape[1:]
        )
        shared_out.start(0)

    later = (iota((count, count), 0) <= iota((count, count), 1)).astype(jnp.bfloat16)
    slots = iota((cap, count), 0).astype(jnp.float32)

    def member(names, expert):
        return jnp.where(jnp.logical_or(names[0:1] == expert, names[1:2] == expert), 1.0, 0.0)

    def seats(mine):
        return jnp.where(mine > 0.0, dot(mine.astype(jnp.bfloat16), later) - 1.0, -1.0)

    def process(*group):
        for i, s in enumerate(group):
            chosen = (slots == ranks[s]).astype(jnp.bfloat16)
            picked[i * cap : (i + 1) * cap, :] = dot(
                chosen, tok[s].reshape(count, features)
            ).astype(jnp.bfloat16)
        a = picked[: len(group) * cap, :]
        for h in range(0, pieces, 2):
            at = slice(h * quarter, h * quarter + half)
            v = dot(a, gate[:, at])
            v = (v / (1.0 + jnp.exp(-v)) * dot(a, up[:, at])).astype(jnp.bfloat16)
            for i, s in enumerate(group):
                for k in range(2):
                    hidden[s, tp, h + k] = v[
                        i * cap : (i + 1) * cap, k * quarter : (k + 1) * quarter
                    ]
                hidden_of(s).start(h)

    def back(s):
        return remote(result.at[s], returned.at[ep], r_send.at[0], r_recv.at[0], ep=s)

    def project(*group, now=True):
        def part(q):
            total = None
            for h in range(pieces):
                a = jnp.concatenate([hidden[s, q, h] for s in group], axis=0)
                one = dot(a, down[q, h])
                total = one if total is None else total + one
            return total

        total = part(tp)
        for s in group:
            hidden_of(s).near()
        for o in range(1, side):
            total = total + part(peers[0, o])
            total = total + part(peers[o, 0])
        for s in group:
            hidden_of(s).far()
        for dy in range(1, side):
            for dx in range(1, side):
                total = total + part(peers[dy, dx])
        for i, s in enumerate(group):
            result[s] = total[i * cap : (i + 1) * cap].astype(jnp.bfloat16)
        if len(group) == 2:
            returned[ep] = result[ep]
            back(mate).start()
        elif now:
            back(group[0]).start()

    def scan_block():
        for copy in loads[4:7]:
            copy.wait()
        column = fill_table(rate_ref, table, states)
        drive_into(x_ref, column, shift_ref, map_ref, table, mag, push_re, push_im, states)
        zero = jnp.zeros((SUBLANES, merged), jnp.float32)
        ends_re, ends_im, product = sweep(table, mag, push_re, push_im, zero, zero, False)
        end = join(table, ends_re, ends_im, product, pre, rows // SUBLANES)
        for i, v in enumerate(end):
            blocks[core, i : i + 1, :] = v

        @pl.when(core == 0)
        def _():
            first_block().start()

    def first_block():
        return remote(blocks.at[0], blocks.at[0], b_send.at[0], b_recv.at[0], ep=mate)

    def whole_chip(d, c):
        return remote(
            summary.at[chip], summary.at[chip], e_send.at[d], e_recv.at[chip],
            ep=lax.rem(2 * (chip + d) + c, n_ep),
        )

    def turn_over(count):
        return power(table[0:1, :], table[1:2, :], count)

    def scan_chip():
        @pl.when(core == 1)
        def _():
            first_block().wait_recv()
            first = blocks[0]
            part = blocks[1]
            re, im = follow(part, turn_over(rows), first[0:1], first[1:2])
            for i, v in enumerate((re, im, first[2:3] * part[2:3])):
                summary[chip, i : i + 1, :] = v
            for d in range(1, chips):
                @pl.when(chip + d < chips)
                def _():
                    for c in range(2):
                        whole_chip(d, c).start()

    def rank(first, number):
        mine = [member(named[first + i], ep) for i in range(number)]
        mine += [mine[0]] * (-number % SUBLANES)
        place = seats(jnp.concatenate(mine, axis=0))
        for i in range(number):
            ranks[first + i] = place[i : i + 1]

    def gain_blocks():
        names = routes_ref[...]
        level = gains_ref[...]
        wanted = [member(names, e) for e in range(n_ep)]
        wanted += [wanted[0]] * (-n_ep % SUBLANES)
        places = seats(jnp.concatenate(wanted, axis=0))
        for e in range(n_ep):
            weight = jnp.where(names[0:1] == e, level[0:1], 0.0) + jnp.where(
                names[1:2] == e, level[1:2], 0.0
            )
            wide = jnp.where(slots == places[e : e + 1], weight, 0.0)
            top, rest = halves(wide)
            high[e * cap : (e + 1) * cap, :] = top
            low[e * cap : (e + 1) * cap, :] = rest

    def scan_states():
        for k in range(chips - 1):
            @pl.when(k < chip)
            def _():
                remote(
                    summary.at[k], summary.at[k], e_send.at[0], e_recv.at[k], ep=mate
                ).wait_recv()

        turn = turn_over(2 * rows)

        def fold(k, carry):
            return follow(summary[k], turn, *carry)

        nothing = jnp.zeros((1, merged), jnp.float32)
        in_re, in_im = lax.fori_loop(0, chip, fold, (nothing, nothing))
        step_re, step_im = follow(blocks[0], turn_over(rows), in_re, in_im)
        in_re = jnp.where(core == 1, step_re, in_re)
        in_im = jnp.where(core == 1, step_im, in_im)
        add_re, add_im = times(pre[2], pre[3], in_re, in_im)
        sweep(table, mag, push_re, push_im, pre[0] + add_re, pre[1] + add_im, True)
        loads[8].wait()
        active[tp] = read_states(readout_ref, push_re, push_im, states).reshape(active.shape[1:])
        active_out.start(0)

    def mix():
        active_out.near()
        active_out.far()
        loads[9].wait()
        total = None
        for q in range(n_tp):
            a = active[q].reshape(rows, channels)
            part = dot(a, weight_ref[q * channels : (q + 1) * channels, :])
            total = part if total is None else total + part
        out_ref[...] = total.astype(out_ref.dtype)
        shared_out.near()
        shared_out.far()
        loads[10].wait()
        width = shared.shape[3]
        total = None
        for q in range(n_tp):
            a = shared[q].reshape(count, width)
            part = dot(a, sdown[q * width : (q + 1) * width, :])
            total = part if total is None else total + part
        common[...] = total

    plan = visits(chips)
    last = len(plan[0]) - 1

    def here(u, field):
        value = jnp.int32(plan[0][u][field])
        for k in range(1, chips):
            value = jnp.where(chip == k, jnp.int32(plan[k][u][field]), value)
        return value

    source = [here(u, 0) for u in range(last + 1)]
    onward = [here(u, 1) for u in range(last + 1)]
    steps = [here(u, 2) for u in range(last + 1)]

    def along(u):
        target = 2 * jnp.maximum(onward[u], 0) + core
        return piece(source[u], core, on_send.at[0], target)

    def aside(u):
        return piece(source[u], core, mate_send.at[0], mate)

    def pass_on(u):
        aside(u).wait_recv()

        @pl.when(onward[u] >= 0)
        def _():
            along(u).start()

        aside(u).start()

    def ready(s):
        piece(s, 1 - core, mate_send.at[0], mate).wait_recv()

    groups = [(2 * chip, 2 * chip + 1)] + [(s,) for s in source]

    def forward(group):
        for s in group:
            hidden_of(s).forward()

    shared_hidden()
    depart(1)
    for copy in loads[2:4]:
        copy.wait()
    ready(mate)
    remote(routes_ref, named.at[mate], n_send.at[0], n_recv.at[0], ep=mate).wait_recv()
    rank(2 * chip, 2)
    process(*groups[0])
    scan_block()
    gain_blocks()
    scan_chip()
    shared_out.forward()
    rest = named.at[pl.ds(0, n_ep - 2)]
    remote(rest, rest, n_send.at[0], n_recv.at[1], ep=mate).wait_recv()
    rank(0, n_ep)

    def arrivals(step):
        for v in range(last + 1):
            if any(units[v][2] == step for units in plan):
                @pl.when(steps[v] == step)
                def _():
                    pass_on(v)

    end = jnp.logical_or(chip == 0, chip == chips - 1)
    for u in range(last + 1):
        arrivals(3 * u)
        if 1 < u == last:
            forward(groups[u])
        ready(source[u])
        process(source[u])
        arrivals(3 * u + 1)
        if u == min(1, last):
            @pl.when(end)
            def _():
                forward(groups[u])

            scan_states()

            @pl.when(jnp.logical_not(end))
            def _():
                forward(groups[u])

        elif u < last:
            forward(groups[u])
        if u == min(2, last):
            active_out.forward()
        if u == 1:
            loads[7].wait()
        if u > 0:
            project(*groups[u - 1], now=u != 2)
        arrivals(3 * u + 2)
        if u == 2:
            back(source[0]).start()
        if u == min(4, last):
            mix()
    project(*groups[last])
    forward(groups[last + 1])
    project(*groups[last + 1])
    rest = returned.at[pl.ds(0, n_ep - 1)]
    remote(rest, rest, r_send.at[0], r_recv.at[0], ep=mate).wait_recv()
    back_rows = returned[...].reshape(n_ep * cap, returned.shape[2])
    routed = dot(high[...], back_rows, TN) + dot(low[...], back_rows, TN)
    experts_ref[...] = (common[...] + routed).astype(experts_ref.dtype)
    shared_out.drain(shared.at[pl.ds(0, n_tp - 1)])
    active_out.drain(active.at[pl.ds(0, n_tp - 1)])
    hidden_of(ep).drain(hidden.at[:, pl.ds(0, n_tp - 1)])

    def drain(at, send, recv):
        remote(at, at, send, recv, ep=mate).wait_send()

    drain(named.at[pl.ds(0, n_ep - 1)], n_send.at[0], n_recv.at[0])

    @pl.when(core == 0)
    def _():
        first_block().wait_send()

    for d in range(1, chips):
        @pl.when(jnp.logical_and(core == 1, chip + d < chips))
        def _():
            drain(summary.at[pl.ds(0, 2)], e_send.at[d], e_recv.at[0])

    drain(result.at[pl.ds(0, n_ep - 1)], r_send.at[0], r_recv.at[0])
    drain(tok.at[:, 0], mate_send.at[0], tok_recv.at[0, 0])
    for d in range(2):
        @pl.when(ends[d][0])
        def _():
            drain(tok.at[pl.ds(0, 2), 0], own_send.at[d], tok_recv.at[0, 0])

    @pl.when(jnp.logical_and(ends[0][0], ends[1][0]))
    def _():
        drain(tok.at[pl.ds(0, last + 1), 0], on_send.at[0], tok_recv.at[0, 0])


def shards(
    mixer_input,
    log_step,
    decay_shift,
    input_map,
    readout,
    mixer_weight,
    expert_input,
    norm_gain,
    routes,
    route_weight,
    expert_switch_matrix,
    up_weight,
    down_weight,
    shared_gate,
    shared_up,
    shared_down,
):
    n_ep, n_tp = lax.axis_size("ep"), lax.axis_size("tp")
    count, features = expert_input.shape
    cap = 2 * count * routes.shape[1] // n_ep
    rows, channels = mixer_input.shape
    groups = log_step.shape[0]
    states, width = input_map.shape[2:]
    merged = groups * states
    f32, bf16 = jnp.float32, jnp.bfloat16
    ff = up_weight.shape[2]
    depth, columns = down_weight.shape[1:]
    shared_ff = shared_up.shape[1]
    vmem = pl.BlockSpec(memory_space=pltpu.VMEM)
    anywhere = pl.BlockSpec(memory_space=pl.ANY)
    dma = pltpu.SemaphoreType.DMA
    operands = (
        routes.T,
        route_weight.T,
        log_step.reshape(1, groups),
        norm_gain.reshape(1, features),
        expert_input.reshape(2, count // 2, features),
        mixer_input,
        decay_shift.T,
        input_map.swapaxes(2, 3).reshape(2, channels, states),
        readout.reshape(2, channels, states),
        mixer_weight,
        shared_gate,
        shared_up,
        shared_down,
        expert_switch_matrix.reshape(features, ff),
        up_weight.reshape(features, ff),
        down_weight.reshape(n_tp, 4, ff // 4, columns),
    )
    return tuple(pl.pallas_call(
        functools.partial(fused_kernel, n_ep, n_tp, states),
        out_shape=(
            pltpu.VMEM((rows, mixer_weight.shape[1]), bf16),
            pltpu.VMEM((count, columns), bf16),
        ),
        in_specs=[anywhere] * len(operands),
        out_specs=(vmem, vmem),
        scratch_shapes=[pltpu.VMEM(a.shape, a.dtype) for a in operands] + [
            pltpu.VMEM((4, merged), f32),
            pltpu.VMEM((rows, merged), f32),
            pltpu.VMEM((rows, merged), f32),
            pltpu.VMEM((rows, merged), f32),
            pltpu.VMEM((4, SUBLANES, merged), f32),
            pltpu.VMEM((2, 3, merged), f32),
            pltpu.VMEM((n_ep // 2, 3, merged), f32),
            pltpu.VMEM((n_tp, 2, rows // 2, channels), bf16),
            pltpu.VMEM((n_ep, 2, count // 2, features), bf16),
            pltpu.VMEM((n_ep, 2, count), jnp.int32),
            pltpu.VMEM((n_ep, 1, count), f32),
            pltpu.VMEM((2 * cap, features), bf16),
            pltpu.VMEM((n_ep, n_tp, 4, cap, ff // 4), bf16),
            pltpu.VMEM((n_ep, cap, columns), bf16),
            pltpu.VMEM((n_ep, cap, columns), bf16),
            pltpu.VMEM((n_tp, 2, count // 2, shared_ff), bf16),
            pltpu.VMEM((count, columns), f32),
            pltpu.VMEM((n_ep * cap, count), bf16),
            pltpu.VMEM((n_ep * cap, count), bf16),
            dma((len(operands),)), dma((n_ep, 2)), dma((1,)), dma((2,)), dma((1,)),
            dma((1,)), dma((2,)), dma((1,)), dma((1,)), dma((n_ep // 2,)), dma((n_ep // 2,)),
            dma((1,)), dma((3,)),
            dma((1,)), dma((n_ep, 4)), dma((1,)), dma((1,)), dma((1,)), dma((3,)),
        ],
        compiler_params=pltpu.CompilerParams(
            collective_id=0, has_side_effects=True, vmem_limit_bytes=56 * 1024 * 1024
        ),
        name="fused",
    )(*operands))


def solution(mesh):
    placed = (
        P("ep", "tp"),
        P("tp"),
        P("ep", "tp"),
        P(None, "tp", None, None),
        P(None, "tp", None, None),
        P(None, "tp"),
        P("ep", None),
        P(),
        P("ep", None),
        P("ep", None),
        P("ep", None, "tp"),
        P("ep", None, "tp"),
        P("ep", None, "tp"),
        P(None, "tp"),
        P(None, "tp"),
        P(None, "tp"),
    )
    return jax.shard_map(
        shards,
        mesh=mesh,
        in_specs=placed,
        out_specs=(P("ep", "tp"), P("ep", "tp")),
        check_vma=False,
    )
```

```python
import functools
import math

import jax
import jax.numpy as jnp
from jax import lax
from jax.experimental import pallas as pl
from jax.experimental.pallas import tpu as pltpu
from jax.sharding import PartitionSpec as P

MESH = pl.DeviceIdType.MESH
SUBLANES = 8
NT = (((1,), (1,)), ((), ()))
TN = (((0,), (0,)), ((), ()))


def times(ar, ai, br, bi):
    return ar * br - ai * bi, ar * bi + ai * br


def iota(shape, dim):
    return lax.broadcasted_iota(jnp.int32, shape, dim)


def spread(shape, period):
    return (iota(shape, 1) % period == iota(shape, 0)).astype(jnp.bfloat16)


def halves(a):
    high = a.astype(jnp.bfloat16)
    return high, (a - high.astype(jnp.float32)).astype(jnp.bfloat16)


def dot(a, b, dims=None):
    if dims is None:
        return jnp.dot(a, b, preferred_element_type=jnp.float32)
    return lax.dot_general(a, b, dims, preferred_element_type=jnp.float32)


def fill_table(rate_ref, table, states):
    groups = rate_ref.shape[1]
    merged = table.shape[1]
    same = iota((groups, groups), 0) == iota((groups, groups), 1)
    column = jnp.sum(jnp.where(same, rate_ref[...], 0.0), axis=1, keepdims=True)
    place = iota((groups, merged), 1) // states == iota((groups, merged), 0)
    wide = jnp.sum(jnp.where(place, column, 0.0), axis=0, keepdims=True)
    step_rate = jnp.exp(wide)
    frequency = jnp.pi * lax.rem(iota((1, merged), 1), states).astype(jnp.float32)
    angle = step_rate * frequency
    turn_cosine = jnp.cos(angle)
    turn_sine = jnp.sin(angle)
    base = jnp.exp(-0.5 * step_rate)
    starting_quadrature = base * turn_sine
    inverse = 1.0 / (0.25 + frequency * frequency)
    lowered = base * turn_cosine - 1.0
    table[0:1, :] = turn_cosine
    table[1:2, :] = turn_sine
    table[2:3, :] = (-0.5 * lowered + starting_quadrature * frequency) * inverse
    table[3:4, :] = (-0.5 * starting_quadrature - lowered * frequency) * inverse
    return column


def drive_into(x_ref, column, shift_ref, map_ref, table_ref, mag, push_re, push_im, states):
    rows, channels = x_ref.shape
    merged = mag.shape[1]
    groups = shift_ref.shape[0]
    width = channels // groups
    steps = rows // SUBLANES
    place = iota((rows, rows), 0)
    order = (iota((rows, rows), 1) == (place % SUBLANES) * steps + place // SUBLANES).astype(
        jnp.bfloat16
    )
    level = jnp.exp(-0.5 * jnp.exp(column) + shift_ref[...])
    high, middle = halves(level)
    low = ((level - high.astype(jnp.float32)) - middle.astype(jnp.float32)).astype(jnp.bfloat16)
    widen = (iota((groups, merged), 1) // states == iota((groups, merged), 0)).astype(jnp.bfloat16)
    total = None
    for piece in (high, middle, low):
        part = dot(dot(order, piece, NT).astype(jnp.bfloat16), widen)
        total = part if total is None else total + part
    mag[...] = total
    x = dot(order, x_ref[...]).astype(jnp.bfloat16)
    repeat = spread((states, merged), states)
    mine = iota((channels, merged), 1) // states == iota((channels, merged), 0) // width
    drives = []
    for c in range(2):
        wide = jnp.where(mine, dot(map_ref[c], repeat), 0.0).astype(jnp.bfloat16)
        drives.append(dot(x, wide))
    re, im = times(table_ref[2:3, :], table_ref[3:4, :], drives[0], drives[1])
    push_re[...] = re
    push_im[...] = im


def sweep(table_ref, mag, push_re, push_im, start_re, start_im, keep):
    rows, merged = mag.shape
    turn_re = jnp.broadcast_to(table_ref[0:1, :], (SUBLANES, merged))
    turn_im = jnp.broadcast_to(table_ref[1:2, :], (SUBLANES, merged))

    def one(j, carry):
        re, im, product = carry
        at = pl.ds(pl.multiple_of(j * SUBLANES, SUBLANES), SUBLANES)
        level = mag[at, :]
        next_re, next_im = times(turn_re, turn_im, re, im)
        next_re = level * next_re + push_re[at, :]
        next_im = level * next_im + push_im[at, :]
        if keep:
            push_re[at, :] = next_re
            push_im[at, :] = next_im
        else:
            product = product * level
        return next_re, next_im, product

    product = jnp.ones((SUBLANES, merged), jnp.float32)
    if keep:
        def pair(j, carry):
            return one(j, carry + (None,))[:2]
        return lax.fori_loop(0, rows // SUBLANES, pair, (start_re, start_im))
    return lax.fori_loop(0, rows // SUBLANES, one, (start_re, start_im, product))


def power(wr, wi, steps):
    reached = 1
    while reached < steps:
        wr, wi = times(wr, wi, wr, wi)
        reached *= 2
    return wr, wi


def join(table_ref, ends_re, ends_im, product, pre, steps):
    merged = ends_re.shape[1]
    wr, wi = power(table_ref[0:1, :], table_ref[1:2, :], steps)
    cr = jnp.zeros((1, merged), jnp.float32)
    ci = cr
    ar = cr + 1.0
    ai = cr
    whole = cr + 1.0
    for s in range(SUBLANES):
        for i, v in enumerate((cr, ci, ar, ai)):
            pre[i, s : s + 1, :] = v
        level = product[s : s + 1]
        fr, fi = level * wr, level * wi
        tr, ti = times(fr, fi, cr, ci)
        cr, ci = tr + ends_re[s : s + 1], ti + ends_im[s : s + 1]
        ar, ai = times(fr, fi, ar, ai)
        whole = whole * level
    return cr, ci, whole


def follow(part, turn, re, im):
    re, im = times(turn[0], turn[1], re, im)
    return part[2:3] * re + part[0:1], part[2:3] * im + part[1:2]


def read_states(readout_ref, push_re, push_im, states):
    rows, merged = push_re.shape
    channels = readout_ref.shape[1]
    width = channels * states // merged
    repeat = spread((states, merged), states)
    mine = iota((channels, merged), 1) // states == iota((channels, merged), 0) // width
    total = None
    for c, ref in enumerate((push_re, push_im)):
        high, low = halves(ref[...])
        back = readout_ref[c] if c == 0 else -readout_ref[c]
        wide_high, wide_low = (
            jnp.where(mine, dot(half, repeat), 0.0).astype(jnp.bfloat16) for half in halves(back)
        )
        part = dot(high, wide_high, NT) + (dot(low, wide_high, NT) + dot(high, wide_low, NT))
        total = part if total is None else total + part
    place = iota((rows, rows), 0)
    steps = rows // SUBLANES
    order = (iota((rows, rows), 1) == (place % steps) * SUBLANES + place // steps).astype(
        jnp.bfloat16
    )
    cube = total + 0.044715 * (total * total * total)
    active = (0.5 * total * (1.0 + jnp.tanh(0.7978845608028654 * cube))).astype(jnp.bfloat16)
    return dot(order, active).astype(jnp.bfloat16)


def remote(src, dst, send, recv, **target):
    return pltpu.make_async_remote_copy(
        src_ref=src, dst_ref=dst, send_sem=send, recv_sem=recv,
        device_id=target, device_id_type=MESH,
    )


def visits(chips):
    plan = []
    for chip in range(chips):
        end = chip in (0, chips - 1)
        found = []
        for d in range(1, chips):
            for j in range(2):
                for there, onward in ((chip - d, chip + 1), (chip + d, chip - 1)):
                    if 0 <= there < chips:
                        onward = onward if 0 <= onward < chips else -1
                        found.append((2 * there + j, onward, 2 * d + j))
        units = []
        for u, (source, onward, arrival) in enumerate(found):
            together = max(v for v in range(len(found)) if found[v][2] == arrival)
            ahead = max((3 * together - 1) // 2, 3 * together - 7) if together > 1 else 0
            units.append((source, onward, 3 * u if end else ahead))
        plan.append(units)
    return plan


def fused_kernel(
    n_ep, n_tp, states,
    routes_hbm, gains_hbm, rate_hbm, gain_hbm, input_hbm, x_hbm, shift_hbm, map_hbm, readout_hbm, weight_hbm,
    sgate_hbm, sup_hbm, sdown_hbm, gate_hbm, up_hbm, down_hbm,
    out_ref, experts_ref,
    routes_ref, gains_ref, rate_ref, gain_ref, tokens, x_ref, shift_ref, map_ref, readout_ref, weight_ref,
    sgate, sup, sdown, gate, up, down,
    table, mag, push_re, push_im, pre, blocks, summary, active,
    tok, named, ranks, picked, hidden, result, returned, shared, common, high, low,
    load, tok_recv, mate_send, own_send, on_send, n_send, n_recv,
    b_send, b_recv, e_send, e_recv, a_send, a_recv, h_send, h_recv, r_send, r_recv, s_send, s_recv,
):
    ep = lax.axis_index("ep")
    tp = lax.axis_index("tp")
    rows, channels = x_ref.shape
    merged = mag.shape[1]
    half_rows, features = tok.shape[2:]
    count = 2 * half_rows
    cap = picked.shape[0] // 2
    chips = n_ep // 2
    chip, core = ep // 2, lax.rem(ep, 2)
    mate = ep + 1 - 2 * core
    side = math.isqrt(n_tp)
    y, x = tp // side, lax.rem(tp, side)
    pieces, quarter = hidden.shape[2], hidden.shape[4]
    half = 2 * quarter

    first_loads = [
        pltpu.make_async_copy(a, b, load.at[i])
        for i, (a, b) in enumerate((
            (input_hbm, tokens), (gain_hbm, gain_ref), (routes_hbm, routes_ref),
            (gains_hbm, gains_ref), (rate_hbm, rate_ref),
        ))
    ]
    for copy in first_loads:
        copy.start()
    barrier = pltpu.get_barrier_semaphore()
    for d in range(1, n_ep):
        pl.semaphore_signal(
            barrier, inc=1, device_id={"ep": lax.rem(ep + d, n_ep)}, device_id_type=MESH
        )
    for d in range(1, n_tp):
        pl.semaphore_signal(
            barrier, inc=1, device_id={"tp": lax.rem(tp + d, n_tp)}, device_id_type=MESH
        )
    pairs = (
        (sgate_hbm, sgate), (sup_hbm, sup), (gate_hbm, gate), (up_hbm, up),
        (x_hbm, x_ref), (shift_hbm, shift_ref), (map_hbm, map_ref), (down_hbm, down),
        (readout_hbm, readout_ref), (weight_hbm, weight_ref), (sdown_hbm, sdown),
    )
    loads = [
        pltpu.make_async_copy(a, b, load.at[len(first_loads) + i])
        for i, (a, b) in enumerate(pairs)
    ]
    for copy in loads:
        copy.start()
    def across(dy, dx):
        return lax.rem(y + dy, side) * side + lax.rem(x + dx, side)

    peers = {(dy, dx): across(dy, dx) for dy in range(side) for dx in range(side)}

    class Share:
        def __init__(self, buffer, send, recv):
            self.buffer, self.send, self.recv = buffer, send, recv
            self.pieces = buffer.shape[1]

        def copy(self, source, h, to, k):
            at = self.buffer.at[source, h]
            return remote(at, at, self.send, self.recv.at[k], tp=to)

        def start(self, h):
            for o in range(1, side):
                self.copy(tp, h, peers[0, o], h // 2).start()
                self.copy(tp, h + 1, peers[o, 0], h // 2).start()
            if h + 2 == self.pieces:
                for g in range(0, self.pieces, 2):
                    for o in range(1, side):
                        self.copy(tp, g + 1, peers[0, o], self.pieces // 2).start()
                        self.copy(tp, g, peers[o, 0], self.pieces // 2).start()

        def wait(self, at, k):
            remote(at, at, self.send, self.recv.at[k], tp=peers[0, 1]).wait_recv()

        def forward(self):
            far = self.pieces // 2 + 1
            for h in range(0, self.pieces, 2):
                self.wait(self.buffer.at[pl.ds(0, side - 1), pl.ds(h, 2)], h // 2)
                for o in range(1, side):
                    for d in range(1, side):
                        self.copy(peers[0, o], h, peers[d, 0], far).start()
                        self.copy(peers[o, 0], h + 1, peers[0, d], far).start()

        def near(self):
            self.wait(self.buffer.at[pl.ds(0, side - 1)], self.pieces // 2)

        def far(self):
            self.wait(self.buffer.at[pl.ds(0, (side - 1) ** 2)], self.pieces // 2 + 1)

        def drain(self, at):
            remote(at, at, self.send, self.recv.at[0], tp=peers[0, 1]).wait_send()

    def hidden_of(s):
        return Share(hidden.at[s], h_send.at[0], h_recv.at[s])

    shared_out = Share(shared, s_send.at[0], s_recv)
    active_out = Share(active, a_send.at[0], a_recv)

    for copy in first_loads:
        copy.wait()
    block = 16
    scale = gain_ref[...]

    @pl.loop(0, half_rows // block)
    def _(i):
        at = pl.ds(pl.multiple_of(i * block, block), block)
        for h in range(2):
            values = tokens[h, at, :].astype(jnp.float32)
            level = lax.rsqrt(jnp.mean(values * values, axis=-1, keepdims=True) + 1e-06)
            tok[ep, h, at, :] = (values * level * scale).astype(jnp.bfloat16)

    named[ep] = routes_ref[...]
    pl.semaphore_wait(barrier, n_ep + n_tp - 2)

    def piece(s, h, send, target):
        return remote(tok.at[s, h], tok.at[s, h], send, tok_recv.at[s, h], ep=target)

    piece(ep, 1 - core, mate_send.at[0], mate).start()
    piece(ep, core, mate_send.at[0], mate).start()
    remote(routes_ref, named.at[ep], n_send.at[0], n_recv.at[0], ep=mate).start()
    strangers = [
        2 * lax.rem(chip + d, chips) + c for d in range(1, chips) for c in range(2)
    ]
    for target in strangers:
        remote(routes_ref, named.at[ep], n_send.at[0], n_recv.at[1], ep=target).start()
    ends = ((chip > 0, lax.rem(ep + n_ep - 2, n_ep)), (chip < chips - 1, lax.rem(ep + 2, n_ep)))

    def own(j, d):
        return piece(2 * chip + j, core, own_send.at[d], ends[d][1])

    def depart(j):
        @pl.when(core != j)
        def _():
            piece(2 * chip + j, core, mate_send.at[0], mate).wait_recv()

        for d in range(2):
            @pl.when(ends[d][0])
            def _():
                own(j, d).start()

    depart(0)

    def shared_hidden():
        for copy in loads[0:2]:
            copy.wait()
        a = tok[ep].reshape(count, features)
        v = dot(a, sgate[...])
        shared[tp] = (v / (1.0 + jnp.exp(-v)) * dot(a, sup[...])).astype(jnp.bfloat16).reshape(
            shared.shape[1:]
        )
        shared_out.start(0)

    later = (iota((count, count), 0) <= iota((count, count), 1)).astype(jnp.bfloat16)
    slots = iota((cap, count), 0).astype(jnp.float32)

    def member(names, expert):
        return jnp.where(jnp.logical_or(names[0:1] == expert, names[1:2] == expert), 1.0, 0.0)

    def seats(mine):
        return jnp.where(mine > 0.0, dot(mine.astype(jnp.bfloat16), later) - 1.0, -1.0)

    def process(*group):
        for i, s in enumerate(group):
            chosen = (slots == ranks[s]).astype(jnp.bfloat16)
            picked[i * cap : (i + 1) * cap, :] = dot(
                chosen, tok[s].reshape(count, features)
            ).astype(jnp.bfloat16)
        a = picked[: len(group) * cap, :]
        for h in range(0, pieces, 2):
            at = slice(h * quarter, h * quarter + half)
            v = dot(a, gate[:, at])
            v = (v / (1.0 + jnp.exp(-v)) * dot(a, up[:, at])).astype(jnp.bfloat16)
            for i, s in enumerate(group):
                for k in range(2):
                    hidden[s, tp, h + k] = v[
                        i * cap : (i + 1) * cap, k * quarter : (k + 1) * quarter
                    ]
                hidden_of(s).start(h)

    def back(s):
        return remote(result.at[s], returned.at[ep], r_send.at[0], r_recv.at[0], ep=s)

    def project(*group, now=True):
        def part(q):
            total = None
            for h in range(pieces):
                a = jnp.concatenate([hidden[s, q, h] for s in group], axis=0)
                one = dot(a, down[q, h])
                total = one if total is None else total + one
            return total

        total = part(tp)
        for s in group:
            hidden_of(s).near()
        for o in range(1, side):
            total = total + part(peers[0, o])
            total = total + part(peers[o, 0])
        for s in group:
            hidden_of(s).far()
        for dy in range(1, side):
            for dx in range(1, side):
                total = total + part(peers[dy, dx])
        for i, s in enumerate(group):
            result[s] = total[i * cap : (i + 1) * cap].astype(jnp.bfloat16)
        if len(group) == 2:
            returned[ep] = result[ep]
            back(mate).start()
        elif now:
            back(group[0]).start()

    def scan_block():
        for copy in loads[4:7]:
            copy.wait()
        column = fill_table(rate_ref, table, states)
        drive_into(x_ref, column, shift_ref, map_ref, table, mag, push_re, push_im, states)
        zero = jnp.zeros((SUBLANES, merged), jnp.float32)
        ends_re, ends_im, product = sweep(table, mag, push_re, push_im, zero, zero, False)
        end = join(table, ends_re, ends_im, product, pre, rows // SUBLANES)
        for i, v in enumerate(end):
            blocks[core, i : i + 1, :] = v

        @pl.when(core == 0)
        def _():
            first_block().start()

    def first_block():
        return remote(blocks.at[0], blocks.at[0], b_send.at[0], b_recv.at[0], ep=mate)

    def whole_chip(d, c):
        return remote(
            summary.at[chip], summary.at[chip], e_send.at[d], e_recv.at[chip],
            ep=lax.rem(2 * (chip + d) + c, n_ep),
        )

    def turn_over(count):
        return power(table[0:1, :], table[1:2, :], count)

    def scan_chip():
        @pl.when(core == 1)
        def _():
            first_block().wait_recv()
            first = blocks[0]
            part = blocks[1]
            re, im = follow(part, turn_over(rows), first[0:1], first[1:2])
            for i, v in enumerate((re, im, first[2:3] * part[2:3])):
                summary[chip, i : i + 1, :] = v
            for d in range(1, chips):
                @pl.when(chip + d < chips)
                def _():
                    for c in range(2):
                        whole_chip(d, c).start()

    def rank(first, number):
        mine = [member(named[first + i], ep) for i in range(number)]
        mine += [mine[0]] * (-number % SUBLANES)
        place = seats(jnp.concatenate(mine, axis=0))
        for i in range(number):
            ranks[first + i] = place[i : i + 1]

    def gain_blocks():
        names = routes_ref[...]
        level = gains_ref[...]
        wanted = [member(names, e) for e in range(n_ep)]
        wanted += [wanted[0]] * (-n_ep % SUBLANES)
        places = seats(jnp.concatenate(wanted, axis=0))
        for e in range(n_ep):
            weight = jnp.where(names[0:1] == e, level[0:1], 0.0) + jnp.where(
                names[1:2] == e, level[1:2], 0.0
            )
            wide = jnp.where(slots == places[e : e + 1], weight, 0.0)
            top, rest = halves(wide)
            high[e * cap : (e + 1) * cap, :] = top
            low[e * cap : (e + 1) * cap, :] = rest

    def scan_states():
        for k in range(chips - 1):
            @pl.when(k < chip)
            def _():
                remote(
                    summary.at[k], summary.at[k], e_send.at[0], e_recv.at[k], ep=mate
                ).wait_recv()

        turn = turn_over(2 * rows)

        def fold(k, carry):
            return follow(summary[k], turn, *carry)

        nothing = jnp.zeros((1, merged), jnp.float32)
        in_re, in_im = lax.fori_loop(0, chip, fold, (nothing, nothing))
        step_re, step_im = follow(blocks[0], turn_over(rows), in_re, in_im)
        in_re = jnp.where(core == 1, step_re, in_re)
        in_im = jnp.where(core == 1, step_im, in_im)
        add_re, add_im = times(pre[2], pre[3], in_re, in_im)
        sweep(table, mag, push_re, push_im, pre[0] + add_re, pre[1] + add_im, True)
        loads[8].wait()
        active[tp] = read_states(readout_ref, push_re, push_im, states).reshape(active.shape[1:])
        active_out.start(0)

    def mix():
        active_out.near()
        active_out.far()
        loads[9].wait()
        total = None
        for q in range(n_tp):
            a = active[q].reshape(rows, channels)
            part = dot(a, weight_ref[q * channels : (q + 1) * channels, :])
            total = part if total is None else total + part
        out_ref[...] = total.astype(out_ref.dtype)
        shared_out.near()
        shared_out.far()
        loads[10].wait()
        width = shared.shape[3]
        total = None
        for q in range(n_tp):
            a = shared[q].reshape(count, width)
            part = dot(a, sdown[q * width : (q + 1) * width, :])
            total = part if total is None else total + part
        common[...] = total

    plan = visits(chips)
    last = len(plan[0]) - 1

    def here(u, field):
        value = jnp.int32(plan[0][u][field])
        for k in range(1, chips):
            value = jnp.where(chip == k, jnp.int32(plan[k][u][field]), value)
        return value

    source = [here(u, 0) for u in range(last + 1)]
    onward = [here(u, 1) for u in range(last + 1)]
    steps = [here(u, 2) for u in range(last + 1)]

    def along(u):
        target = 2 * jnp.maximum(onward[u], 0) + core
        return piece(source[u], core, on_send.at[0], target)

    def aside(u):
        return piece(source[u], core, mate_send.at[0], mate)

    def pass_on(u):
        aside(u).wait_recv()

        @pl.when(onward[u] >= 0)
        def _():
            along(u).start()

        aside(u).start()

    def ready(s):
        piece(s, 1 - core, mate_send.at[0], mate).wait_recv()

    groups = [(2 * chip, 2 * chip + 1)] + [(s,) for s in source]

    def forward(group):
        for s in group:
            hidden_of(s).forward()

    shared_hidden()
    depart(1)
    for copy in loads[2:4]:
        copy.wait()
    ready(mate)
    remote(routes_ref, named.at[mate], n_send.at[0], n_recv.at[0], ep=mate).wait_recv()
    rank(2 * chip, 2)
    process(*groups[0])
    scan_block()
    gain_blocks()
    scan_chip()
    shared_out.forward()
    rest = named.at[pl.ds(0, n_ep - 2)]
    remote(rest, rest, n_send.at[0], n_recv.at[1], ep=mate).wait_recv()
    rank(0, n_ep)

    def arrivals(step):
        for v in range(last + 1):
            if any(units[v][2] == step for units in plan):
                @pl.when(steps[v] == step)
                def _():
                    pass_on(v)

    end = jnp.logical_or(chip == 0, chip == chips - 1)
    for u in range(last + 1):
        arrivals(3 * u)
        if 1 < u == last:
            forward(groups[u])
        elif u == last - 1 > 1:
            @pl.when(end)
            def _():
                forward(groups[u])

        ready(source[u])
        process(source[u])
        arrivals(3 * u + 1)
        if u == min(1, last):
            @pl.when(end)
            def _():
                forward(groups[u])

            scan_states()

            @pl.when(jnp.logical_not(end))
            def _():
                forward(groups[u])

        elif u == last - 1:
            @pl.when(jnp.logical_not(end))
            def _():
                forward(groups[u])

        elif u < last:
            forward(groups[u])
        if u == min(2, last):
            active_out.forward()
        if u == 1:
            loads[7].wait()
        if u > 0:
            project(*groups[u - 1], now=u != 2)
        arrivals(3 * u + 2)
        if u == 2:
            back(source[0]).start()
        if u == min(4, last):
            mix()
    project(*groups[last])
    forward(groups[last + 1])
    project(*groups[last + 1])
    rest = returned.at[pl.ds(0, n_ep - 1)]
    remote(rest, rest, r_send.at[0], r_recv.at[0], ep=mate).wait_recv()
    back_rows = returned[...].reshape(n_ep * cap, returned.shape[2])
    routed = dot(high[...], back_rows, TN) + dot(low[...], back_rows, TN)
    experts_ref[...] = (common[...] + routed).astype(experts_ref.dtype)
    shared_out.drain(shared.at[pl.ds(0, n_tp - 1)])
    active_out.drain(active.at[pl.ds(0, n_tp - 1)])
    hidden_of(ep).drain(hidden.at[:, pl.ds(0, n_tp - 1)])

    def drain(at, send, recv):
        remote(at, at, send, recv, ep=mate).wait_send()

    drain(named.at[pl.ds(0, n_ep - 1)], n_send.at[0], n_recv.at[0])

    @pl.when(core == 0)
    def _():
        first_block().wait_send()

    for d in range(1, chips):
        @pl.when(jnp.logical_and(core == 1, chip + d < chips))
        def _():
            drain(summary.at[pl.ds(0, 2)], e_send.at[d], e_recv.at[0])

    drain(result.at[pl.ds(0, n_ep - 1)], r_send.at[0], r_recv.at[0])
    drain(tok.at[:, 0], mate_send.at[0], tok_recv.at[0, 0])
    for d in range(2):
        @pl.when(ends[d][0])
        def _():
            drain(tok.at[pl.ds(0, 2), 0], own_send.at[d], tok_recv.at[0, 0])

    @pl.when(jnp.logical_and(ends[0][0], ends[1][0]))
    def _():
        drain(tok.at[pl.ds(0, last + 1), 0], on_send.at[0], tok_recv.at[0, 0])


def shards(
    mixer_input,
    log_step,
    decay_shift,
    input_map,
    readout,
    mixer_weight,
    expert_input,
    norm_gain,
    routes,
    route_weight,
    expert_switch_matrix,
    up_weight,
    down_weight,
    shared_gate,
    shared_up,
    shared_down,
):
    n_ep, n_tp = lax.axis_size("ep"), lax.axis_size("tp")
    count, features = expert_input.shape
    cap = 2 * count * routes.shape[1] // n_ep
    rows, channels = mixer_input.shape
    groups = log_step.shape[0]
    states, width = input_map.shape[2:]
    merged = groups * states
    f32, bf16 = jnp.float32, jnp.bfloat16
    ff = up_weight.shape[2]
    depth, columns = down_weight.shape[1:]
    shared_ff = shared_up.shape[1]
    vmem = pl.BlockSpec(memory_space=pltpu.VMEM)
    anywhere = pl.BlockSpec(memory_space=pl.ANY)
    dma = pltpu.SemaphoreType.DMA
    operands = (
        routes.T,
        route_weight.T,
        log_step.reshape(1, groups),
        norm_gain.reshape(1, features),
        expert_input.reshape(2, count // 2, features),
        mixer_input,
        decay_shift.T,
        input_map.swapaxes(2, 3).reshape(2, channels, states),
        readout.reshape(2, channels, states),
        mixer_weight,
        shared_gate,
        shared_up,
        shared_down,
        expert_switch_matrix.reshape(features, ff),
        up_weight.reshape(features, ff),
        down_weight.reshape(n_tp, 4, ff // 4, columns),
    )
    return tuple(pl.pallas_call(
        functools.partial(fused_kernel, n_ep, n_tp, states),
        out_shape=(
            pltpu.VMEM((rows, mixer_weight.shape[1]), bf16),
            pltpu.VMEM((count, columns), bf16),
        ),
        in_specs=[anywhere] * len(operands),
        out_specs=(vmem, vmem),
        scratch_shapes=[pltpu.VMEM(a.shape, a.dtype) for a in operands] + [
            pltpu.VMEM((4, merged), f32),
            pltpu.VMEM((rows, merged), f32),
            pltpu.VMEM((rows, merged), f32),
            pltpu.VMEM((rows, merged), f32),
            pltpu.VMEM((4, SUBLANES, merged), f32),
            pltpu.VMEM((2, 3, merged), f32),
            pltpu.VMEM((n_ep // 2, 3, merged), f32),
            pltpu.VMEM((n_tp, 2, rows // 2, channels), bf16),
            pltpu.VMEM((n_ep, 2, count // 2, features), bf16),
            pltpu.VMEM((n_ep, 2, count), jnp.int32),
            pltpu.VMEM((n_ep, 1, count), f32),
            pltpu.VMEM((2 * cap, features), bf16),
            pltpu.VMEM((n_ep, n_tp, 4, cap, ff // 4), bf16),
            pltpu.VMEM((n_ep, cap, columns), bf16),
            pltpu.VMEM((n_ep, cap, columns), bf16),
            pltpu.VMEM((n_tp, 2, count // 2, shared_ff), bf16),
            pltpu.VMEM((count, columns), f32),
            pltpu.VMEM((n_ep * cap, count), bf16),
            pltpu.VMEM((n_ep * cap, count), bf16),
            dma((len(operands),)), dma((n_ep, 2)), dma((1,)), dma((2,)), dma((1,)),
            dma((1,)), dma((2,)), dma((1,)), dma((1,)), dma((n_ep // 2,)), dma((n_ep // 2,)),
            dma((1,)), dma((3,)),
            dma((1,)), dma((n_ep, 4)), dma((1,)), dma((1,)), dma((1,)), dma((3,)),
        ],
        compiler_params=pltpu.CompilerParams(
            collective_id=0, has_side_effects=True, vmem_limit_bytes=56 * 1024 * 1024
        ),
        name="fused",
    )(*operands))


def solution(mesh):
    placed = (
        P("ep", "tp"),
        P("tp"),
        P("ep", "tp"),
        P(None, "tp", None, None),
        P(None, "tp", None, None),
        P(None, "tp"),
        P("ep", None),
        P(),
        P("ep", None),
        P("ep", None),
        P("ep", None, "tp"),
        P("ep", None, "tp"),
        P("ep", None, "tp"),
        P(None, "tp"),
        P(None, "tp"),
        P(None, "tp"),
    )
    return jax.shard_map(
        shards,
        mesh=mesh,
        in_specs=placed,
        out_specs=(P("ep", "tp"), P("ep", "tp")),
        check_vma=False,
    )
```
